1024 devices in a mesh: sp: 128 (over z, y), tp: 8 (over x, core).
Axes of the slice: x: 4, y: 8, z: 16, core: 2. Of those that a mesh axis runs over, the one named last changes fastest.
Arguments:
- glu_value: bfloat16 [65536, 1024], P('sp', 'tp'), may hold values from -6 to 6
- glu_gate: bfloat16 [65536, 1024], P('sp', 'tp'), may hold values from -8 to 8
- conv_taps: bfloat16 [31, 1024], P(None, 'tp'), may hold values from -1 to 1
- norm_gain: float32 [1024], P('tp'), may hold values from 0.1 to 1.9
- out_weight: bfloat16 [2048, 1024], P(None, 'tp'), may hold values from -0.1875 to 0.1875
- norm_mean: float32 [65536], P('sp'), may hold values from -3 to 3
- norm_scale: float32 [65536], P('sp'), may hold values from 0.5 to 2
- out_grad: bfloat16 [65536, 2048], P('sp'), may hold values from -24 to 24
Outputs:
- value_grad: bfloat16 [65536, 1024], P('sp', 'tp')
- gate_grad: bfloat16 [65536, 1024], P('sp', 'tp')
- taps_grad: float32 [31, 1024], P(None, 'tp')
- gain_grad: float32 [1024], P('tp')
- weight_grad: float32 [2048, 1024], P('sp', 'tp')
The draws below stay inside these ranges and needn't reach their ends.
All inputs are finite; a program needn't handle non-finite values.
Results may differ from the reference program's by a relative error of at most 0.0047.
Values may be sent and summed in bfloat16 or wider, within the bound.
No kernel may reach another device: no remote copies, remote signals or barrier semaphores. Data moves between devices by JAX's collectives and lax.ppermute only.
A program may use at most 32 MiB of HBM per device.

```python
import math
import jax
import jax.numpy as jnp
from jax import lax

D = 2048
CH = 1024
KW = 31
TOKENS = 65536


def spiked(drawn, stream_key, source, target, parts, factor):
    owner, partner = [(jnp.arange(drawn.shape[position]) // (drawn.shape[position] // parts)).reshape([-1 if axis == position else 1 for axis in range(drawn.ndim)]) for position in (source, target)]
    chosen = jax.random.permutation(stream_key, parts)[partner]
    strong = (owner == chosen) | (owner == (partner + parts // 2) % parts)
    return jnp.where(strong, factor * drawn, drawn)


def levels(rng, shape, pieces, smallest, largest):
    level = 1.0
    for axis_at, blocks in pieces:
        steps = jax.random.uniform(jax.random.fold_in(jax.random.fold_in(rng, 6), axis_at), (blocks,), jnp.float32, smallest / len(pieces), largest / len(pieces))
        level = level * jnp.repeat(jnp.exp(steps), shape[axis_at] // blocks).reshape((-1,) + (1,) * (len(shape) - 1 - axis_at))
    return level


def centred(own_key, dims, deviation, most, pieces=(), dtype=jnp.bfloat16):
    values = jax.random.normal(own_key, dims, jnp.float32) * deviation
    if len(pieces) > 0:
        values = levels(own_key, dims, pieces, -0.22, 0.18) * values
    return jnp.clip(values, min=-most, max=most).astype(dtype)


def gaussian_with(stream_key, dims, spread, bound, pieces, heavy, dtype=jnp.bfloat16):
    drawn = spread * jax.random.normal(stream_key, dims, jnp.float32)
    if pieces:
        drawn = drawn * levels(stream_key, dims, pieces, -0.22, 0.18)
    return jnp.clip(spiked(drawn, jax.random.fold_in(stream_key, 3), *heavy), -bound, bound).astype(dtype)


def setup_inputs(seed: int = 0) -> dict:
    arg_keys = jax.random.split(jax.random.key(seed), 9)
    return {
        "glu_value": centred(arg_keys[0], (TOKENS, CH), 1.0, 6.0, ((0, 128), (1, 8))),
        "glu_gate": centred(arg_keys[1], (TOKENS, CH), 1.5, 8.0, ((0, 128), (1, 8))),
        "conv_taps": centred(arg_keys[2], (KW, CH), KW ** -0.5, 1.0, ((1, 8),)),
        "norm_gain": jnp.clip(1.0 + 0.18 * jax.random.normal(arg_keys[3], (CH,), jnp.float32), 0.1, 1.9),
        "out_weight": centred(arg_keys[4], (D, CH), CH ** -0.5, 0.1875, ((1, 8),)),
        "norm_mean": centred(arg_keys[5], (TOKENS,), 0.3, 3.0, ((0, 128),), jnp.float32),
        "norm_scale": jnp.clip(jnp.exp(math.log(2.0) - 1.3862944 * jax.random.uniform(arg_keys[6], (TOKENS,), jnp.float32) ** levels(arg_keys[6], (TOKENS,), ((0, 128),), -0.2, 0.2)), 0.5, 2.0),
        "out_grad": gaussian_with(arg_keys[7], (TOKENS, D), 1.0, 24.0, ((0, 128),), (0, 1, 128, 5.5)),
    }


def reference(glu_value, glu_gate, conv_taps, norm_gain, out_weight, norm_mean, norm_scale, out_grad):
    val_float = glu_value.astype(jnp.float32)
    gate_sig = jax.nn.sigmoid(glu_gate.astype(jnp.float32))
    gated = (val_float * gate_sig).astype(jnp.bfloat16)
    padded = jnp.pad(gated.astype(jnp.float32), ((KW - 1, 0), (0, 0)))
    taps_float = conv_taps.astype(jnp.float32)
    conv = jnp.zeros((TOKENS, CH), jnp.float32)
    for offset in range(KW):
        conv = conv + taps_float[offset] * padded[offset:offset + TOKENS]
    centered = (conv - norm_mean[:, None]) * norm_scale[:, None]
    normed = centered * norm_gain
    sig_norm = jax.nn.sigmoid(normed)
    activated = (normed * sig_norm).astype(jnp.bfloat16)
    act_grad = jnp.dot(out_grad, out_weight, preferred_element_type=jnp.float32)
    normed_grad = act_grad * sig_norm * (1.0 + normed * (1.0 - sig_norm))
    gain_grad = jnp.sum(normed_grad * centered, axis=0)
    scaled_grad = normed_grad * norm_gain
    mean_plain = jnp.mean(scaled_grad, axis=1)
    mean_cross = jnp.mean(scaled_grad * centered, axis=1)
    conv_grad = norm_scale[:, None] * (scaled_grad - mean_plain[:, None] - centered * mean_cross[:, None])
    grad_padded = jnp.pad(conv_grad, ((0, KW - 1), (0, 0)))
    gated_grad = jnp.zeros((TOKENS, CH), jnp.float32)
    tap_list = []
    for offset in range(KW):
        begin = KW - 1 - offset
        gated_grad = gated_grad + taps_float[offset] * grad_padded[begin:begin + TOKENS]
        tap_list.append(jnp.sum(conv_grad * padded[offset:offset + TOKENS], axis=0))
    taps_grad = jnp.stack(tap_list, axis=0)
    value_grad = (gated_grad * gate_sig).astype(jnp.bfloat16)
    gate_grad = (gated_grad * val_float * gate_sig * (1.0 - gate_sig)).astype(jnp.bfloat16)
    weight_grad = lax.dot_general(out_grad, activated, (((0,), (0,)), ((), ())), preferred_element_type=jnp.float32)
    return value_grad, gate_grad, taps_grad, gain_grad, weight_grad
```

```python
import jax
import jax.numpy as jnp
from jax import lax
from jax.sharding import Mesh
from jax.sharding import PartitionSpec as P

CH = 1024
SP = ("z", "y")


def passed_along(value, axis, by):
    length = lax.axis_size(axis)
    pairs = [(i, i + by) for i in range(length) if 0 <= i + by < length]
    return lax.ppermute(value, axis, pairs)


def exchange(value, axis):
    return lax.all_to_all(value, axis, split_axis=0, concat_axis=0, tiled=True)


def to_all(value, axis):
    copies = jnp.broadcast_to(value, (lax.axis_size(axis), *value.shape))
    return exchange(copies, axis)


def per_device(
    glu_value, glu_gate, conv_taps, norm_gain, out_weight, norm_mean, norm_scale, out_grad
):
    f32, bf16 = jnp.float32, jnp.bfloat16
    tok_rows, chans = glu_value.shape
    reach_back = conv_taps.shape[0] - 1
    n_z, n_y = lax.axis_size("z"), lax.axis_size("y")
    val_float = glu_value.astype(f32)
    gate_sig = jax.nn.sigmoid(glu_gate.astype(f32))
    gated = (val_float * gate_sig).astype(bf16)
    before = passed_along(gated[tok_rows - reach_back :], SP, 1)
    padded = jnp.concatenate([before, gated], axis=0).astype(f32)
    taps_float = conv_taps.astype(f32)
    conv = jnp.zeros(gated.shape, f32)
    for offset in range(reach_back + 1):
        conv = conv + taps_float[offset] * padded[offset : offset + tok_rows]
    centered = (conv - norm_mean[:, None]) * norm_scale[:, None]
    normed = centered * norm_gain
    sig_norm = jax.nn.sigmoid(normed)
    activated = (normed * sig_norm).astype(bf16)
    act_grad = jnp.dot(out_grad, out_weight, preferred_element_type=f32)
    normed_grad = act_grad * sig_norm * (1.0 + normed * (1.0 - sig_norm))
    gain_local = jnp.sum(normed_grad * centered, axis=0)
    scaled_grad = normed_grad * norm_gain
    sums = jnp.stack([jnp.sum(scaled_grad, axis=1), jnp.sum(scaled_grad * centered, axis=1)])
    sums = to_all(sums.reshape(1, -1), "tp").sum(axis=0).reshape(2, tok_rows)
    mean_plain = sums[0] / CH
    mean_cross = sums[1] / CH
    weight_part = lax.dot_general(
        out_grad, activated, (((0,), (0,)), ((), ())), preferred_element_type=f32
    )
    own_rows = weight_part.shape[0] // (n_z * n_y)
    weight_part = weight_part.astype(bf16).reshape(n_z, n_y, own_rows, chans)
    weight_part = weight_part.transpose(1, 0, 2, 3).reshape(n_y, n_z * own_rows, chans)
    weight_part = exchange(weight_part, "y").astype(f32).sum(axis=0)

    conv_grad = norm_scale[:, None] * (
        scaled_grad - mean_plain[:, None] - centered * mean_cross[:, None]
    )
    after = passed_along(conv_grad[:reach_back], SP, -1)
    grad_padded = jnp.concatenate([conv_grad, after], axis=0)
    gated_grad = jnp.zeros(conv_grad.shape, f32)
    tap_list = []
    for offset in range(reach_back + 1):
        begin = reach_back - offset
        gated_grad = gated_grad + taps_float[offset] * grad_padded[begin : begin + tok_rows]
        tap_list.append(jnp.sum(conv_grad * padded[offset : offset + tok_rows], axis=0))
    small = jnp.stack([*tap_list, gain_local], axis=0)
    small = to_all(small, "y").sum(axis=0).astype(bf16)
    value_grad = (gated_grad * gate_sig).astype(bf16)
    gate_grad = (gated_grad * val_float * gate_sig * (1.0 - gate_sig)).astype(bf16)

    last = jnp.concatenate(
        [
            weight_part.astype(bf16).reshape(n_z, own_rows, chans),
            jnp.broadcast_to(small, (n_z, *small.shape)),
        ],
        axis=1,
    )
    last = exchange(last, "z").astype(f32).sum(axis=0)
    weight_grad = last[:own_rows]
    taps_grad = last[own_rows : own_rows + reach_back + 1]
    gain_grad = last[own_rows + reach_back + 1]
    return (value_grad, gate_grad, taps_grad, gain_grad, weight_grad)


def solution(mesh):
    torus = Mesh(mesh.devices.reshape(16, 8, mesh.shape["tp"]), ("z", "y", "tp"))
    placed = (
        P(SP, "tp"),
        P(SP, "tp"),
        P(None, "tp"),
        P("tp"),
        P(None, "tp"),
        P(SP),
        P(SP),
        P(SP, None),
    )
    return jax.shard_map(
        per_device,
        mesh=torus,
        in_specs=placed,
        out_specs=(P(SP, "tp"), P(SP, "tp"), P(None, "tp"), P("tp"), P(SP, "tp")),
        check_vma=False,
    )
```

```python
import jax
import jax.numpy as jnp
from jax import lax
from jax.sharding import Mesh
from jax.sharding import PartitionSpec as P

CH = 1024
SP = ("z", "y")


def passed_along(value, axis, by):
    length = lax.axis_size(axis)
    pairs = [(i, i + by) for i in range(length) if 0 <= i + by < length]
    return lax.ppermute(value, axis, pairs)


def exchange(value, axis):
    return lax.all_to_all(value, axis, split_axis=0, concat_axis=0, tiled=True)


def to_all(value, axis):
    copies = jnp.broadcast_to(value, (lax.axis_size(axis), *value.shape))
    return exchange(copies, axis)


def per_device(
    glu_value, glu_gate, conv_taps, norm_gain, out_weight, norm_mean, norm_scale, out_grad
):
    f32, bf16 = jnp.float32, jnp.bfloat16
    tok_rows, chans = glu_value.shape
    reach_back = conv_taps.shape[0] - 1
    n_z, n_y = lax.axis_size("z"), lax.axis_size("y")
    val_float = glu_value.astype(f32)
    gate_sig = jax.nn.sigmoid(glu_gate.astype(f32))
    gated = (val_float * gate_sig).astype(bf16)
    last_rows = lax.optimization_barrier(
        (glu_value[tok_rows - reach_back :], glu_gate[tok_rows - reach_back :])
    )
    last_gated = last_rows[0].astype(f32) * jax.nn.sigmoid(last_rows[1].astype(f32))
    before = passed_along(last_gated.astype(bf16), SP, 1)
    padded = jnp.concatenate([before, gated], axis=0).astype(f32)
    taps_float = conv_taps.astype(f32)
    conv = jnp.zeros(gated.shape, f32)
    for offset in range(reach_back + 1):
        conv = conv + taps_float[offset] * padded[offset : offset + tok_rows]
    centered = (conv - norm_mean[:, None]) * norm_scale[:, None]
    normed = centered * norm_gain
    sig_norm = jax.nn.sigmoid(normed)
    activated = (normed * sig_norm).astype(bf16)
    act_grad = jnp.dot(out_grad, out_weight, preferred_element_type=f32)
    normed_grad = act_grad * sig_norm * (1.0 + normed * (1.0 - sig_norm))
    gain_local = jnp.sum(normed_grad * centered, axis=0)
    scaled_grad = normed_grad * norm_gain
    sums = jnp.stack([jnp.sum(scaled_grad, axis=1), jnp.sum(scaled_grad * centered, axis=1)])
    sums = to_all(sums.reshape(1, -1), "tp").sum(axis=0).reshape(2, tok_rows)
    mean_plain = sums[0] / CH
    mean_cross = sums[1] / CH
    weight_part = lax.dot_general(
        out_grad, activated, (((0,), (0,)), ((), ())), preferred_element_type=f32
    )
    own_rows = weight_part.shape[0] // (n_z * n_y)
    weight_part = weight_part.astype(bf16).reshape(n_z, n_y, own_rows, chans)
    weight_part = weight_part.transpose(1, 0, 2, 3).reshape(n_y, n_z * own_rows, chans)

    conv_grad = norm_scale[:, None] * (
        scaled_grad - mean_plain[:, None] - centered * mean_cross[:, None]
    )
    after = passed_along(conv_grad[:reach_back], SP, -1)
    grad_padded = jnp.concatenate([conv_grad, after], axis=0)
    gated_grad = jnp.zeros(conv_grad.shape, f32)
    tap_list = []
    for offset in range(reach_back + 1):
        begin = reach_back - offset
        gated_grad = gated_grad + taps_float[offset] * grad_padded[begin : begin + tok_rows]
        tap_list.append(jnp.sum(conv_grad * padded[offset : offset + tok_rows], axis=0))
    small = jnp.stack([*tap_list, gain_local], axis=0).astype(bf16)
    n_big = n_z * own_rows
    both = jnp.concatenate(
        [weight_part, jnp.broadcast_to(small, (n_y, *small.shape))], axis=1
    )
    both = exchange(both, "y").astype(f32).sum(axis=0).astype(bf16)
    value_grad = (gated_grad * gate_sig).astype(bf16)
    gate_grad = (gated_grad * val_float * gate_sig * (1.0 - gate_sig)).astype(bf16)

    last = jnp.concatenate(
        [
            both[:n_big].reshape(n_z, own_rows, chans),
            jnp.broadcast_to(both[n_big:], (n_z, *small.shape)),
        ],
        axis=1,
    )
    last = exchange(last, "z").astype(f32).sum(axis=0)
    weight_grad = last[:own_rows]
    taps_grad = last[own_rows : own_rows + reach_back + 1]
    gain_grad = last[own_rows + reach_back + 1]
    return (value_grad, gate_grad, taps_grad, gain_grad, weight_grad)


def solution(mesh):
    torus = Mesh(mesh.devices.reshape(16, 8, mesh.shape["tp"]), ("z", "y", "tp"))
    placed = (
        P(SP, "tp"),
        P(SP, "tp"),
        P(None, "tp"),
        P("tp"),
        P(None, "tp"),
        P(SP),
        P(SP),
        P(SP, None),
    )
    return jax.shard_map(
        per_device,
        mesh=torus,
        in_specs=placed,
        out_specs=(P(SP, "tp"), P(SP, "tp"), P(None, "tp"), P("tp"), P(SP, "tp")),
        check_vma=False,
    )
```

```python
import functools

import jax
import jax.numpy as jnp
from jax import lax
from jax.experimental import pallas as pl
from jax.experimental.pallas import tpu as pltpu
from jax.sharding import Mesh
from jax.sharding import PartitionSpec as P

SP = ("z", "y")
HALO = 32
BLOCK = 64
LANES = 128
F32, BF16 = jnp.float32, jnp.bfloat16
VMEM = pl.BlockSpec(memory_space=pltpu.VMEM)
HBM = pl.BlockSpec(memory_space=pltpu.HBM)


def column(row):
    return jnp.transpose(jnp.broadcast_to(row, (LANES, LANES)))


def row_sums(block):
    return jnp.sum(jnp.transpose(block), axis=0, keepdims=True)


def weighted(taps_ref, source_ref, first, rows, step):
    total = None
    for k in range(taps_ref.shape[0] - 1):
        begin = first + step * k
        term = taps_ref[k : k + 1, :] * source_ref[begin : begin + rows, :]
        total = term if total is None else total + term
    return total


def silu_parts(conv, mean, scale, gain, act_grad):
    centered = (conv - mean) * scale
    normed = centered * gain
    sig = jax.nn.sigmoid(normed)
    normed_grad = act_grad * sig * (1.0 + normed * (1.0 - sig))
    return centered, (normed * sig).astype(BF16), normed_grad, normed_grad * gain


def tail_kernel(value_ref, gate_ref, out_ref, value_rows, gate_rows, sems):
    first = value_ref.shape[0] - HALO
    copies = [
        pltpu.make_async_copy(ref.at[pl.ds(first, HALO)], rows, sems.at[i])
        for i, (ref, rows) in enumerate(((value_ref, value_rows), (gate_ref, gate_rows)))
    ]
    for c in copies:
        c.start()
    for c in copies:
        c.wait()
    sig = jax.nn.sigmoid(gate_rows[...].astype(F32))
    out_ref[...] = (value_rows[...].astype(F32) * sig).astype(BF16)


def main_kernel(
    value_in, gate_in, taps_in, gain_in, mean_in, scale_in, weight_in, out_grad_in,
    taps, gain_ref, mean_ref, scale_ref, out_grad_ref,
    gated_ref, centered_ref, scaled_ref, activated_ref, conv_first, act_first, gain_sum, sums_ref,
    value_ref, gate_ref, padded, taps_raw, weight_ref, conv_ref, sems,
):
    rows, taps_n = value_ref.shape[0], taps_in.shape[0]
    moved = (
        (value_in, value_ref), (gate_in, gate_ref), (taps_in, taps_raw), (gain_in, gain_ref),
        (mean_in, mean_ref), (scale_in, scale_ref), (weight_in, weight_ref),
        (out_grad_in, out_grad_ref),
    )
    copies = [pltpu.make_async_copy(src, dst, sems.at[i]) for i, (src, dst) in enumerate(moved)]
    for c in copies:
        c.start()
    for c in copies[:3]:
        c.wait()
    taps[0:taps_n, :] = taps_raw[...].astype(F32)
    gated = (value_ref[...].astype(F32) * jax.nn.sigmoid(gate_ref[...].astype(F32))).astype(BF16)
    gated_ref[...] = gated
    padded[0:HALO, :] = jnp.zeros((HALO, LANES), F32)
    padded[HALO : HALO + rows, :] = gated.astype(F32)
    for r in range(0, rows, BLOCK):
        conv_ref[r : r + BLOCK, :] = weighted(taps, padded, 2 + r, BLOCK, 1)
    for c in copies[3:]:
        c.wait()
    conv_first[...] = conv_ref[0:HALO, :]
    gain = gain_ref[...]
    gain_total = jnp.zeros((8, LANES), F32)
    n_b = rows // LANES
    for b in range(n_b):
        at = b * LANES
        mean, scale = column(mean_ref[b : b + 1, :]), column(scale_ref[b : b + 1, :])
        act_grad = jnp.dot(
            out_grad_ref[at : at + LANES, :], weight_ref[...], preferred_element_type=F32
        )
        if b == 0:
            act_first[...] = act_grad[:HALO]
        plain, cross = [], []
        for h in range(0, LANES, BLOCK):
            r = at + h
            centered, activated, normed_grad, scaled = silu_parts(
                conv_ref[r : r + BLOCK, :], mean[h : h + BLOCK], scale[h : h + BLOCK], gain,
                act_grad[h : h + BLOCK],
            )
            centered_ref[r : r + BLOCK, :] = centered
            scaled_ref[r : r + BLOCK, :] = scaled
            activated_ref[r : r + BLOCK, :] = activated
            for_gain = normed_grad * centered
            if r == 0:
                for_gain = for_gain[HALO:]
            gain_total += jnp.sum(for_gain.reshape(-1, 8, LANES), axis=0)
            plain.append(scaled)
            cross.append(scaled * centered)
        sums_ref[b : b + 1, :] = row_sums(jnp.concatenate(plain, axis=0))
        sums_ref[n_b + b : n_b + b + 1, :] = row_sums(jnp.concatenate(cross, axis=0))
    gain_sum[...] = gain_total


def first_kernel(
    before_ref, conv_first, act_first, taps, gain_ref, mean_ref, scale_ref, gain_sum, sums_ref,
    centered_ref, scaled_ref, activated_ref, gain_out, sums_out,
    padded,
):
    padded[0:HALO, :] = before_ref[...].astype(F32)
    padded[HALO : 2 * HALO, :] = jnp.zeros((HALO, LANES), F32)
    conv = conv_first[...] + weighted(taps, padded, 2, HALO, 1)
    mean, scale = column(mean_ref[0:1, :])[:HALO], column(scale_ref[0:1, :])[:HALO]
    centered, activated, normed_grad, scaled = silu_parts(
        conv, mean, scale, gain_ref[...], act_first[...]
    )
    centered_ref[...] = centered
    scaled_ref[...] = scaled
    activated_ref[...] = activated
    gain_out[...] = gain_sum[...] + jnp.sum((normed_grad * centered).reshape(-1, 8, LANES), axis=0)
    filler = jnp.zeros((LANES - HALO, LANES), F32)
    plain = row_sums(jnp.concatenate([scaled, filler], axis=0))
    cross = row_sums(jnp.concatenate([scaled * centered, filler], axis=0))
    tile = sums_ref[...]
    n_b = tile.shape[0] // 2
    at_row = lax.broadcasted_iota(jnp.int32, tile.shape, 0)
    mine = lax.broadcasted_iota(jnp.int32, tile.shape, 1) < HALO
    tile = jnp.where((at_row == 0) & mine, plain, tile)
    tile = jnp.where((at_row == n_b) & mine, cross, tile)
    for j in range(sums_out.shape[0]):
        sums_out[j] = tile


def weight_kernel(out_grad_ref, activated_ref, activated_first, out_ref, *, n_z, n_y):
    activated = jnp.concatenate([activated_first[...], activated_ref[HALO:, :]], axis=0)
    part = lax.dot_general(
        out_grad_ref[...], activated, (((0,), (0,)), ((), ())), preferred_element_type=F32
    ).astype(BF16)
    own = part.shape[0] // (n_z * n_y)
    for z in range(n_z):
        for y in range(n_y):
            at = (z * n_y + y) * own
            out_ref[y, z * own : (z + 1) * own, :] = part[at : at + own]


def pack_kernel(
    all_sums, centered_ref, scaled_ref, centered_first, scaled_first, gated_ref, before_ref,
    scale_ref, part_ref, gain_sum,
    out_ref, conv_grad_ref, first_rows, padded,
    *, channels, taps_n,
):
    rows = gated_ref.shape[0]
    tile = all_sums[0]
    for j in range(1, all_sums.shape[0]):
        tile = tile + all_sums[j]
    tile = tile * (1.0 / channels)
    n_b = rows // LANES
    padded[0:HALO, :] = before_ref[...].astype(F32)
    padded[HALO : HALO + rows, :] = gated_ref[...].astype(F32)
    for b in range(n_b):
        at = b * LANES
        plain, cross = column(tile[b : b + 1]), column(tile[n_b + b : n_b + b + 1])
        scale = column(scale_ref[b : b + 1, :])
        centered, scaled = centered_ref[at : at + LANES, :], scaled_ref[at : at + LANES, :]
        if b == 0:
            centered = jnp.concatenate([centered_first[...], centered[HALO:]], axis=0)
            scaled = jnp.concatenate([scaled_first[...], scaled[HALO:]], axis=0)
        conv_grad_ref[at : at + LANES, :] = scale * (scaled - plain - centered * cross)
    first_rows[...] = conv_grad_ref[0:HALO, :]
    small = []
    for k0 in range(0, taps_n, 8):
        ks = range(k0, min(k0 + 8, taps_n))
        totals = {k: jnp.zeros((8, LANES), F32) for k in ks}
        for r in range(0, rows, 8):
            grad = conv_grad_ref[r : r + 8, :]
            for k in ks:
                totals[k] = totals[k] + grad * padded[2 + k + r : 10 + k + r, :]
        small += [jnp.sum(totals[k], axis=0, keepdims=True) for k in ks]
    small.append(jnp.sum(gain_sum[...], axis=0, keepdims=True))
    small = jnp.concatenate(small, axis=0).astype(BF16)
    big = part_ref.shape[1]
    for y in range(out_ref.shape[0]):
        out_ref[y, 0:big, :] = part_ref[y]
        out_ref[y, big : big + taps_n + 1, :] = small


def middle_kernel(in_ref, out_ref, *, own):
    total = in_ref[0].astype(F32)
    for y in range(1, in_ref.shape[0]):
        total = total + in_ref[y].astype(F32)
    total = total.astype(BF16)
    n_z = out_ref.shape[0]
    small = total[n_z * own :]
    for z in range(n_z):
        out_ref[z, 0:own, :] = total[z * own : (z + 1) * own]
        out_ref[z, own:, :] = small


def last_kernel(in_ref, weight_ref, taps_ref, gain_ref):
    total = in_ref[0].astype(F32)
    for z in range(1, in_ref.shape[0]):
        total = total + in_ref[z].astype(F32)
    own, taps_n = weight_ref.shape[0], taps_ref.shape[0]
    weight_ref[...] = total[0:own]
    taps_ref[...] = total[own : own + taps_n]
    gain_ref[...] = total[own + taps_n : own + taps_n + 1]


def glu_kernel(
    value_in, gate_in, conv_grad_ref, after_ref, taps, value_grad, gate_grad,
    value_ref, gate_ref, padded, sems,
):
    rows, taps_n = value_ref.shape[0], taps.shape[0] - 1
    moved = ((value_in, value_ref), (gate_in, gate_ref))
    copies = [pltpu.make_async_copy(src, dst, sems.at[i]) for i, (src, dst) in enumerate(moved)]
    for c in copies:
        c.start()
    padded[0:rows, :] = conv_grad_ref[...]
    padded[rows : rows + HALO, :] = after_ref[...]
    for c in copies:
        c.wait()
    for r in range(0, rows, BLOCK):
        gated_grad = weighted(taps, padded, r + taps_n - 1, BLOCK, -1)
        sig = jax.nn.sigmoid(gate_ref[r : r + BLOCK, :].astype(F32))
        value = value_ref[r : r + BLOCK, :].astype(F32)
        value_grad[r : r + BLOCK, :] = (gated_grad * sig).astype(BF16)
        gate_grad[r : r + BLOCK, :] = (gated_grad * value * sig * (1.0 - sig)).astype(BF16)


def passed_along(value, axis, by):
    length = lax.axis_size(axis)
    pairs = [(i, i + by) for i in range(length) if 0 <= i + by < length]
    return lax.ppermute(value, axis, pairs)


def exchange(value, axis):
    return lax.all_to_all(value, axis, split_axis=0, concat_axis=0, tiled=True)


def call(kernel, outs, in_specs, scratch=(), flops=0, final=False):
    run = pl.pallas_call(
        kernel,
        out_shape=[jax.ShapeDtypeStruct(*o) if final else pltpu.VMEM(*o) for o in outs],
        in_specs=in_specs,
        out_specs=[VMEM] * len(outs),
        scratch_shapes=list(scratch),
        cost_estimate=pl.CostEstimate(flops=flops, bytes_accessed=0, transcendentals=0),
        compiler_params=pltpu.CompilerParams(vmem_limit_bytes=16 << 20),
    )

    def with_operands(*operands):
        return run(
            *(
                pltpu.with_memory_space_constraint(x, spec.memory_space)
                for x, spec in zip(operands, in_specs)
            )
        )

    return with_operands


def per_device(
    glu_value, glu_gate, conv_taps, norm_gain, out_weight, norm_mean, norm_scale, out_grad
):
    rows, chans = glu_value.shape
    taps_n = conv_taps.shape[0]
    wide = out_grad.shape[1]
    n_z, n_y, n_tp = lax.axis_size("z"), lax.axis_size("y"), lax.axis_size("tp")
    own = wide // (n_z * n_y)
    n_b = rows // LANES
    gain = norm_gain.reshape(1, chans)
    mean, scale = norm_mean.reshape(n_b, LANES), norm_scale.reshape(n_b, LANES)
    full, few = (rows, chans), (HALO, chans)

    (tail,) = call(
        tail_kernel, [(few, BF16)], [HBM, HBM],
        [pltpu.VMEM(few, BF16), pltpu.VMEM(few, BF16), pltpu.SemaphoreType.DMA((2,))],
    )(glu_value, glu_gate)
    before = passed_along(tail, SP, 1)
    block = (n_b, LANES)
    (taps, gain, mean, scale, out_grad_here,
     gated, centered, scaled, activated, conv0, act0, gain_sum, sums) = call(
        main_kernel,
        [((taps_n + 1, chans), F32), ((1, chans), F32), (block, F32),
         (block, F32), ((rows, wide), BF16),
         (full, BF16), (full, F32), (full, F32), (full, BF16), (few, F32), (few, F32),
         ((8, chans), F32), ((2 * n_b, LANES), F32)],
        [HBM] * 8,
        [pltpu.VMEM(full, BF16), pltpu.VMEM(full, BF16),
         pltpu.VMEM((HALO + rows, chans), F32), pltpu.VMEM((taps_n, chans), BF16),
         pltpu.VMEM((wide, chans), BF16), pltpu.VMEM(full, F32), pltpu.SemaphoreType.DMA((8,))],
        flops=1 << 28,
    )(glu_value, glu_gate, conv_taps, gain, mean, scale, out_weight, out_grad)
    centered0, scaled0, activated0, gain_sum, sums = call(
        first_kernel,
        [(few, F32), (few, F32), (few, BF16), ((8, chans), F32), ((n_tp, 2 * n_b, LANES), F32)],
        [VMEM] * 9,
        [pltpu.VMEM((2 * HALO, chans), F32)],
        flops=1 << 24,
    )(before, conv0, act0, taps, gain, mean, scale, gain_sum, sums)
    sums = exchange(sums, "tp")
    (part,) = call(
        functools.partial(weight_kernel, n_z=n_z, n_y=n_y),
        [((n_y, n_z * own, chans), BF16)], [VMEM] * 3, flops=1 << 28,
    )(out_grad_here, activated, activated0)
    packed, conv_grad, first_rows = call(
        functools.partial(pack_kernel, channels=chans * n_tp, taps_n=taps_n),
        [((n_y, n_z * own + taps_n + 1, chans), BF16), (full, F32), (few, F32)],
        [VMEM] * 10,
        [pltpu.VMEM((HALO + rows, chans), F32)],
        flops=1 << 26,
    )(sums, centered, scaled, centered0, scaled0, gated, before, scale, part, gain_sum)
    packed = exchange(packed, "y")
    (packed,) = call(
        functools.partial(middle_kernel, own=own),
        [((n_z, own + taps_n + 1, chans), BF16)], [VMEM], flops=1 << 22,
    )(packed)
    packed = exchange(packed, "z")
    after = passed_along(first_rows, SP, -1)
    value_grad, gate_grad = call(
        glu_kernel, [(full, BF16), (full, BF16)], [HBM] * 2 + [VMEM] * 3,
        [pltpu.VMEM(full, BF16), pltpu.VMEM(full, BF16), pltpu.VMEM((rows + HALO, chans), F32),
         pltpu.SemaphoreType.DMA((2,))], flops=1 << 28, final=True,
    )(glu_value, glu_gate, conv_grad, after, taps)
    weight_grad, taps_grad, gain_grad = call(
        last_kernel,
        [((own, chans), F32), ((taps_n, chans), F32), ((1, chans), F32)], [VMEM], flops=1 << 22,
        final=True,
    )(packed)
    return (value_grad, gate_grad, taps_grad, gain_grad.reshape(chans), weight_grad)


def solution(mesh):
    shape = (16, 8) if mesh.shape["sp"] == 128 else (mesh.shape["sp"] // 2, 2)
    torus = Mesh(mesh.devices.reshape(*shape, mesh.shape["tp"]), ("z", "y", "tp"))
    placed = (
        P(SP, "tp"),
        P(SP, "tp"),
        P(None, "tp"),
        P("tp"),
        P(None, "tp"),
        P(SP),
        P(SP),
        P(SP, None),
    )

    return jax.shard_map(
        per_device,
        mesh=torus,
        in_specs=placed,
        out_specs=(P(SP, "tp"), P(SP, "tp"), P(None, "tp"), P("tp"), P(SP, "tp")),
        check_vma=False,
    )
```

```python
import functools

import jax
import jax.numpy as jnp
from jax import lax
from jax.experimental import pallas as pl
from jax.experimental.pallas import tpu as pltpu
from jax.sharding import Mesh
from jax.sharding import PartitionSpec as P

SP = ("z", "y")
HALO = 32
BLOCK = 64
LANES = 128
F32, BF16 = jnp.float32, jnp.bfloat16
VMEM = pl.BlockSpec(memory_space=pltpu.VMEM)
HBM = pl.BlockSpec(memory_space=pltpu.HBM)


def column(row):
    return jnp.transpose(jnp.broadcast_to(row, (LANES, LANES)))


def row_sums(block):
    return jnp.sum(jnp.transpose(block), axis=0, keepdims=True)


def weighted(taps_ref, source_ref, first, rows, step):
    total = None
    for k in range(taps_ref.shape[0] - 1):
        begin = first + step * k
        term = taps_ref[k : k + 1, :] * source_ref[begin : begin + rows, :]
        total = term if total is None else total + term
    return total


def silu_parts(conv, mean, scale, gain, act_grad):
    centered = (conv - mean) * scale
    normed = centered * gain
    sig = jax.nn.sigmoid(normed)
    normed_grad = act_grad * sig * (1.0 + normed * (1.0 - sig))
    return centered, (normed * sig).astype(BF16), normed_grad, normed_grad * gain


def tail_kernel(value_ref, gate_ref, out_ref, value_rows, gate_rows, sems):
    first = value_ref.shape[0] - HALO
    copies = [
        pltpu.make_async_copy(ref.at[pl.ds(first, HALO)], rows, sems.at[i])
        for i, (ref, rows) in enumerate(((value_ref, value_rows), (gate_ref, gate_rows)))
    ]
    for c in copies:
        c.start()
    for c in copies:
        c.wait()
    sig = jax.nn.sigmoid(gate_rows[...].astype(F32))
    out_ref[...] = (value_rows[...].astype(F32) * sig).astype(BF16)


def main_kernel(
    value_ref, gate_ref, taps_raw, gain_ref, mean_ref, scale_ref, weight_ref, out_grad_ref,
    taps, gated_ref, centered_ref, scaled_ref, activated_ref, conv_first, act_first, gain_sum,
    sums_ref, padded, conv_ref,
):
    rows, taps_n = value_ref.shape[0], taps_raw.shape[0]
    taps[0:taps_n, :] = taps_raw[...].astype(F32)
    gated = (value_ref[...].astype(F32) * jax.nn.sigmoid(gate_ref[...].astype(F32))).astype(BF16)
    gated_ref[...] = gated
    padded[0:HALO, :] = jnp.zeros((HALO, LANES), F32)
    padded[HALO : HALO + rows, :] = gated.astype(F32)
    for r in range(0, rows, BLOCK):
        conv_ref[r : r + BLOCK, :] = weighted(taps, padded, 2 + r, BLOCK, 1)
    conv_first[...] = conv_ref[0:HALO, :]
    gain = gain_ref[...]
    gain_total = jnp.zeros((8, LANES), F32)
    n_b = rows // LANES
    for b in range(n_b):
        at = b * LANES
        mean, scale = column(mean_ref[b : b + 1, :]), column(scale_ref[b : b + 1, :])
        act_grad = jnp.dot(
            out_grad_ref[at : at + LANES, :], weight_ref[...], preferred_element_type=F32
        )
        if b == 0:
            act_first[...] = act_grad[:HALO]
        plain, cross = [], []
        for h in range(0, LANES, BLOCK):
            r = at + h
            centered, activated, normed_grad, scaled = silu_parts(
                conv_ref[r : r + BLOCK, :], mean[h : h + BLOCK], scale[h : h + BLOCK], gain,
                act_grad[h : h + BLOCK],
            )
            centered_ref[r : r + BLOCK, :] = centered
            scaled_ref[r : r + BLOCK, :] = scaled
            activated_ref[r : r + BLOCK, :] = activated
            for_gain = normed_grad * centered
            if r == 0:
                for_gain = for_gain[HALO:]
            gain_total += jnp.sum(for_gain.reshape(-1, 8, LANES), axis=0)
            plain.append(scaled)
            cross.append(scaled * centered)
        sums_ref[b : b + 1, :] = row_sums(jnp.concatenate(plain, axis=0))
        sums_ref[n_b + b : n_b + b + 1, :] = row_sums(jnp.concatenate(cross, axis=0))
    gain_sum[...] = gain_total


def first_kernel(
    before_ref, conv_first, act_first, taps, gain_ref, mean_ref, scale_ref, gain_sum, sums_ref,
    centered_ref, scaled_ref, activated_ref, gain_out, sums_out,
    padded,
):
    padded[0:HALO, :] = before_ref[...].astype(F32)
    padded[HALO : 2 * HALO, :] = jnp.zeros((HALO, LANES), F32)
    conv = conv_first[...] + weighted(taps, padded, 2, HALO, 1)
    mean, scale = column(mean_ref[0:1, :])[:HALO], column(scale_ref[0:1, :])[:HALO]
    centered, activated, normed_grad, scaled = silu_parts(
        conv, mean, scale, gain_ref[...], act_first[...]
    )
    centered_ref[...] = centered
    scaled_ref[...] = scaled
    activated_ref[...] = activated
    gain_out[...] = gain_sum[...] + jnp.sum((normed_grad * centered).reshape(-1, 8, LANES), axis=0)
    filler = jnp.zeros((LANES - HALO, LANES), F32)
    plain = row_sums(jnp.concatenate([scaled, filler], axis=0))
    cross = row_sums(jnp.concatenate([scaled * centered, filler], axis=0))
    tile = sums_ref[...]
    n_b = tile.shape[0] // 2
    at_row = lax.broadcasted_iota(jnp.int32, tile.shape, 0)
    mine = lax.broadcasted_iota(jnp.int32, tile.shape, 1) < HALO
    tile = jnp.where((at_row == 0) & mine, plain, tile)
    tile = jnp.where((at_row == n_b) & mine, cross, tile)
    for j in range(sums_out.shape[0]):
        sums_out[j] = tile


def weight_kernel(
    out_grad_ref, activated_ref, activated_first, keep_ref, send_ref, *, n_z, n_y
):
    activated = jnp.concatenate([activated_first[...], activated_ref[HALO:, :]], axis=0)
    part = lax.dot_general(
        out_grad_ref[...], activated, (((0,), (0,)), ((), ())), preferred_element_type=F32
    )
    own = part.shape[0] // (n_z * n_y)
    half = own // 2
    even = jnp.full((half, part.shape[1]), lax.axis_index("z") & 1, jnp.int32) == 0
    for z in range(n_z):
        for y in range(n_y):
            at = (z * n_y + y) * own
            upper, lower = part[at : at + half], part[at + half : at + own]
            keep_ref[y, z * half : (z + 1) * half, :] = jnp.where(even, upper, lower)
            send_ref[y, z * half : (z + 1) * half, :] = jnp.where(even, lower, upper).astype(BF16)


def pack_kernel(
    all_sums, centered_ref, scaled_ref, centered_first, scaled_first, gated_ref, before_ref,
    scale_ref, keep_ref, sent_ref, gain_sum, value_in, gate_in,
    out_ref, conv_grad_ref, first_rows, value_ref, gate_ref, padded, sems,
    *, channels, taps_n,
):
    rows = gated_ref.shape[0]
    moved = ((value_in, value_ref), (gate_in, gate_ref))
    copies = [pltpu.make_async_copy(src, dst, sems.at[i]) for i, (src, dst) in enumerate(moved)]
    for c in copies:
        c.start()
    tile = all_sums[0]
    for j in range(1, all_sums.shape[0]):
        tile = tile + all_sums[j]
    tile = tile * (1.0 / channels)
    n_b = rows // LANES
    padded[0:HALO, :] = before_ref[...].astype(F32)
    padded[HALO : HALO + rows, :] = gated_ref[...].astype(F32)
    for b in range(n_b):
        at = b * LANES
        plain, cross = column(tile[b : b + 1]), column(tile[n_b + b : n_b + b + 1])
        scale = column(scale_ref[b : b + 1, :])
        centered, scaled = centered_ref[at : at + LANES, :], scaled_ref[at : at + LANES, :]
        if b == 0:
            centered = jnp.concatenate([centered_first[...], centered[HALO:]], axis=0)
            scaled = jnp.concatenate([scaled_first[...], scaled[HALO:]], axis=0)
        conv_grad_ref[at : at + LANES, :] = scale * (scaled - plain - centered * cross)
    first_rows[...] = conv_grad_ref[0:HALO, :]
    small = []
    for k0 in range(0, taps_n, 8):
        ks = range(k0, min(k0 + 8, taps_n))
        totals = {k: jnp.zeros((8, LANES), F32) for k in ks}
        for r in range(0, rows, 8):
            grad = conv_grad_ref[r : r + 8, :]
            for k in ks:
                totals[k] = totals[k] + grad * padded[2 + k + r : 10 + k + r, :]
        small += [jnp.sum(totals[k], axis=0, keepdims=True) for k in ks]
    small.append(jnp.sum(gain_sum[...], axis=0, keepdims=True))
    small = jnp.concatenate(small, axis=0).astype(BF16)
    big = keep_ref.shape[1]
    for y in range(out_ref.shape[0]):
        out_ref[y, 0:big, :] = (keep_ref[y] + sent_ref[y].astype(F32)).astype(BF16)
        out_ref[y, big : big + taps_n + 1, :] = small
    for c in copies:
        c.wait()


def middle_kernel(in_ref, out_ref, *, half):
    total = in_ref[0].astype(F32)
    for y in range(1, in_ref.shape[0]):
        total = total + in_ref[y].astype(F32)
    n_z = out_ref.shape[0]
    small = total[n_z * half :].astype(BF16)
    for z in range(n_z):
        out_ref[z, 0:half, :] = total[z * half : (z + 1) * half].astype(BF16)
        out_ref[z, half:, :] = small


def last_kernel(in_ref, weight_ref, taps_ref, gain_ref):
    half, taps_n = weight_ref.shape[0] // 2, taps_ref.shape[0]
    big, small = [], None
    for z in range(in_ref.shape[0]):
        block = in_ref[z].astype(F32)
        if z < 2:
            big.append(block[:half])
        else:
            big[z % 2] = big[z % 2] + block[:half]
        small = block[half:] if small is None else small + block[half:]
    weight_ref[0:half, :] = big[0]
    weight_ref[half:, :] = big[1]
    taps_ref[...] = small[0:taps_n]
    gain_ref[...] = small[taps_n : taps_n + 1]


def glu_kernel(
    value_ref, gate_ref, conv_grad_ref, after_ref, taps, value_grad, gate_grad, padded
):
    rows, taps_n = value_ref.shape[0], taps.shape[0] - 1
    padded[0:rows, :] = conv_grad_ref[...]
    padded[rows : rows + HALO, :] = after_ref[...]
    for r in range(0, rows, BLOCK):
        gated_grad = weighted(taps, padded, r + taps_n - 1, BLOCK, -1)
        sig = jax.nn.sigmoid(gate_ref[r : r + BLOCK, :].astype(F32))
        value = value_ref[r : r + BLOCK, :].astype(F32)
        value_grad[r : r + BLOCK, :] = (gated_grad * sig).astype(BF16)
        gate_grad[r : r + BLOCK, :] = (gated_grad * value * sig * (1.0 - sig)).astype(BF16)


def passed_along(value, axis, by):
    length = lax.axis_size(axis)
    pairs = [(i, i + by) for i in range(length) if 0 <= i + by < length]
    return lax.ppermute(value, axis, pairs)


def exchange(value, axis):
    return lax.all_to_all(value, axis, split_axis=0, concat_axis=0, tiled=True)


def call(kernel, outs, in_specs, scratch=(), flops=0, final=False):
    run = pl.pallas_call(
        kernel,
        out_shape=[jax.ShapeDtypeStruct(*o) if final else pltpu.VMEM(*o) for o in outs],
        in_specs=in_specs,
        out_specs=[VMEM] * len(outs),
        scratch_shapes=list(scratch),
        cost_estimate=pl.CostEstimate(flops=flops, bytes_accessed=0, transcendentals=0),
        compiler_params=pltpu.CompilerParams(vmem_limit_bytes=16 << 20),
    )

    def with_operands(*operands):
        return run(
            *(
                pltpu.with_memory_space_constraint(x, spec.memory_space)
                for x, spec in zip(operands, in_specs)
            )
        )

    return with_operands


def per_device(
    glu_value, glu_gate, conv_taps, norm_gain, out_weight, norm_mean, norm_scale, out_grad
):
    rows, chans = glu_value.shape
    taps_n = conv_taps.shape[0]
    wide = out_grad.shape[1]
    n_z, n_y, n_tp = lax.axis_size("z"), lax.axis_size("y"), lax.axis_size("tp")
    own = wide // (n_z * n_y)
    half = own // 2
    n_b = rows // LANES
    gain = norm_gain.reshape(1, chans)
    mean, scale = norm_mean.reshape(n_b, LANES), norm_scale.reshape(n_b, LANES)
    full, few = (rows, chans), (HALO, chans)

    (tail,) = call(
        tail_kernel, [(few, BF16)], [HBM, HBM],
        [pltpu.VMEM(few, BF16), pltpu.VMEM(few, BF16), pltpu.SemaphoreType.DMA((2,))],
        flops=1 << 30,
    )(glu_value, glu_gate)
    before = passed_along(tail, SP, 1)
    (taps, gated, centered, scaled, activated, conv0, act0, gain_sum, sums) = call(
        main_kernel,
        [((taps_n + 1, chans), F32), (full, BF16), (full, F32), (full, F32), (full, BF16),
         (few, F32), (few, F32), ((8, chans), F32), ((2 * n_b, LANES), F32)],
        [VMEM] * 8,
        [pltpu.VMEM((HALO + rows, chans), F32), pltpu.VMEM(full, F32)],
        flops=1 << 28,
    )(glu_value, glu_gate, conv_taps, gain, mean, scale, out_weight, out_grad)
    centered0, scaled0, activated0, gain_sum, sums = call(
        first_kernel,
        [(few, F32), (few, F32), (few, BF16), ((8, chans), F32), ((n_tp, 2 * n_b, LANES), F32)],
        [VMEM] * 9,
        [pltpu.VMEM((2 * HALO, chans), F32)],
        flops=1 << 24,
    )(before, conv0, act0, taps, gain, mean, scale, gain_sum, sums)
    keep, send = call(
        functools.partial(weight_kernel, n_z=n_z, n_y=n_y),
        [((n_y, n_z * half, chans), F32), ((n_y, n_z * half, chans), BF16)],
        [VMEM] * 3, flops=1 << 28,
    )(out_grad, activated, activated0)
    sent = lax.ppermute(send, "z", [(i, i ^ 1) for i in range(n_z)])
    sums = exchange(sums, "tp")
    packed, conv_grad, first_rows, value, gate = call(
        functools.partial(pack_kernel, channels=chans * n_tp, taps_n=taps_n),
        [((n_y, n_z * half + taps_n + 1, chans), BF16), (full, F32), (few, F32), (full, BF16),
         (full, BF16)],
        [VMEM] * 11 + [HBM] * 2,
        [pltpu.VMEM((HALO + rows, chans), F32), pltpu.SemaphoreType.DMA((2,))],
        flops=1 << 26,
    )(sums, centered, scaled, centered0, scaled0, gated, before, scale, keep, sent, gain_sum,
      glu_value, glu_gate)
    packed = exchange(packed, "y")
    (packed,) = call(
        functools.partial(middle_kernel, half=half),
        [((n_z, half + taps_n + 1, chans), BF16)], [VMEM], flops=1 << 22,
    )(packed)
    packed = exchange(packed, "z")
    after = passed_along(first_rows, SP, -1)
    value_grad, gate_grad = call(
        glu_kernel, [(full, BF16), (full, BF16)], [VMEM] * 5,
        [pltpu.VMEM((rows + HALO, chans), F32)], flops=1 << 28, final=True,
    )(value, gate, conv_grad, after, taps)
    weight_grad, taps_grad, gain_grad = call(
        last_kernel,
        [((own, chans), F32), ((taps_n, chans), F32), ((1, chans), F32)], [VMEM], flops=1 << 22,
        final=True,
    )(packed)
    return (value_grad, gate_grad, taps_grad, gain_grad.reshape(chans), weight_grad)


def solution(mesh):
    shape = (16, 8) if mesh.shape["sp"] == 128 else (mesh.shape["sp"] // 2, 2)
    torus = Mesh(mesh.devices.reshape(*shape, mesh.shape["tp"]), ("z", "y", "tp"))
    placed = (
        P(SP, "tp"),
        P(SP, "tp"),
        P(None, "tp"),
        P("tp"),
        P(None, "tp"),
        P(SP),
        P(SP),
        P(SP, None),
    )

    return jax.shard_map(
        per_device,
        mesh=torus,
        in_specs=placed,
        out_specs=(P(SP, "tp"), P(SP, "tp"), P(None, "tp"), P("tp"), P(SP, "tp")),
        check_vma=False,
    )
```

```python
import functools

import jax
import jax.numpy as jnp
from jax import lax
from jax.experimental import pallas as pl
from jax.experimental.pallas import tpu as pltpu
from jax.sharding import Mesh
from jax.sharding import PartitionSpec as P

SP = ("z", "y")
HALO = 32
BLOCK = 64
LANES = 128
Z_FIRST, Y_FIRST, TP_FIRST = 9, 4, 5
F32, BF16 = jnp.float32, jnp.bfloat16
VMEM = pl.BlockSpec(memory_space=pltpu.VMEM)
HBM = pl.BlockSpec(memory_space=pltpu.HBM)


def column(row):
    return jnp.transpose(jnp.broadcast_to(row, (LANES, LANES)))


def row_sums(block):
    return jnp.sum(jnp.transpose(block), axis=0, keepdims=True)


def weighted(taps_ref, source_ref, first, rows, step):
    total = None
    for k in range(taps_ref.shape[0] - 1):
        begin = first + step * k
        term = taps_ref[k : k + 1, :] * source_ref[begin : begin + rows, :]
        total = term if total is None else total + term
    return total


def silu_parts(conv, mean, scale, gain, act_grad):
    centered = (conv - mean) * scale
    normed = centered * gain
    sig = jax.nn.sigmoid(normed)
    normed_grad = act_grad * sig * (1.0 + normed * (1.0 - sig))
    return centered, (normed * sig).astype(BF16), normed_grad, normed_grad * gain


def tail_kernel(value_ref, gate_ref, out_ref, value_rows, gate_rows, sems):
    first = value_ref.shape[0] - HALO
    copies = [
        pltpu.make_async_copy(ref.at[pl.ds(first, HALO)], rows, sems.at[i])
        for i, (ref, rows) in enumerate(((value_ref, value_rows), (gate_ref, gate_rows)))
    ]
    for c in copies:
        c.start()
    for c in copies:
        c.wait()
    sig = jax.nn.sigmoid(gate_rows[...].astype(F32))
    out_ref[...] = (value_rows[...].astype(F32) * sig).astype(BF16)


def main_kernel(
    value_ref, gate_ref, taps_raw, gain_ref, mean_ref, scale_ref, weight_ref, out_grad_ref,
    taps, gated_ref, centered_ref, scaled_ref, activated_ref, conv_first, act_first, gain_sum,
    sums_ref, padded, conv_ref,
):
    rows, taps_n = value_ref.shape[0], taps_raw.shape[0]
    taps[0:taps_n, :] = taps_raw[...].astype(F32)
    gated = (value_ref[...].astype(F32) * jax.nn.sigmoid(gate_ref[...].astype(F32))).astype(BF16)
    gated_ref[...] = gated
    padded[0:HALO, :] = jnp.zeros((HALO, LANES), F32)
    padded[HALO : HALO + rows, :] = gated.astype(F32)
    for r in range(0, rows, BLOCK):
        conv_ref[r : r + BLOCK, :] = weighted(taps, padded, 2 + r, BLOCK, 1)
    conv_first[...] = conv_ref[0:HALO, :]
    gain = gain_ref[...]
    gain_total = jnp.zeros((8, LANES), F32)
    n_b = rows // LANES
    for b in range(n_b):
        at = b * LANES
        mean, scale = column(mean_ref[b : b + 1, :]), column(scale_ref[b : b + 1, :])
        act_grad = jnp.dot(
            out_grad_ref[at : at + LANES, :], weight_ref[...], preferred_element_type=F32
        )
        if b == 0:
            act_first[...] = act_grad[:HALO]
        plain, cross = [], []
        for h in range(0, LANES, BLOCK):
            r = at + h
            centered, activated, normed_grad, scaled = silu_parts(
                conv_ref[r : r + BLOCK, :], mean[h : h + BLOCK], scale[h : h + BLOCK], gain,
                act_grad[h : h + BLOCK],
            )
            centered_ref[r : r + BLOCK, :] = centered
            scaled_ref[r : r + BLOCK, :] = scaled
            activated_ref[r : r + BLOCK, :] = activated
            for_gain = normed_grad * centered
            if r == 0:
                for_gain = for_gain[HALO:]
            gain_total += jnp.sum(for_gain.reshape(-1, 8, LANES), axis=0)
            plain.append(scaled)
            cross.append(scaled * centered)
        sums_ref[b : b + 1, :] = row_sums(jnp.concatenate(plain, axis=0))
        sums_ref[n_b + b : n_b + b + 1, :] = row_sums(jnp.concatenate(cross, axis=0))
    gain_sum[...] = gain_total


def first_kernel(
    before_ref, conv_first, act_first, taps, gain_ref, mean_ref, scale_ref, gain_sum, sums_ref,
    centered_ref, scaled_ref, activated_ref, gain_out, sums_out,
    padded,
):
    padded[0:HALO, :] = before_ref[...].astype(F32)
    padded[HALO : 2 * HALO, :] = jnp.zeros((HALO, LANES), F32)
    conv = conv_first[...] + weighted(taps, padded, 2, HALO, 1)
    mean, scale = column(mean_ref[0:1, :])[:HALO], column(scale_ref[0:1, :])[:HALO]
    centered, activated, normed_grad, scaled = silu_parts(
        conv, mean, scale, gain_ref[...], act_first[...]
    )
    centered_ref[...] = centered
    scaled_ref[...] = scaled
    activated_ref[...] = activated
    gain_out[...] = gain_sum[...] + jnp.sum((normed_grad * centered).reshape(-1, 8, LANES), axis=0)
    filler = jnp.zeros((LANES - HALO, LANES), F32)
    plain = row_sums(jnp.concatenate([scaled, filler], axis=0))
    cross = row_sums(jnp.concatenate([scaled * centered, filler], axis=0))
    tile = sums_ref[...]
    n_b = tile.shape[0] // 2
    at_row = lax.broadcasted_iota(jnp.int32, tile.shape, 0)
    mine = lax.broadcasted_iota(jnp.int32, tile.shape, 1) < HALO
    tile = jnp.where((at_row == 0) & mine, plain, tile)
    tile = jnp.where((at_row == n_b) & mine, cross, tile)
    for j in range(sums_out.shape[0]):
        sums_out[j] = tile


def weight_kernel(
    out_grad_ref, activated_ref, activated_first, keep_ref, send_ref, *, n_z, n_y
):
    activated = jnp.concatenate([activated_first[...], activated_ref[HALO:, :]], axis=0)
    part = lax.dot_general(
        out_grad_ref[...], activated, (((0,), (0,)), ((), ())), preferred_element_type=F32
    )
    own = part.shape[0] // (n_z * n_y)
    half = own // 2
    even = jnp.full((half, part.shape[1]), lax.axis_index("z") & 1, jnp.int32) == 0
    for z in range(n_z):
        for y in range(n_y):
            at = (z * n_y + y) * own
            upper, lower = part[at : at + half], part[at + half : at + own]
            keep_ref[y, z * half : (z + 1) * half, :] = jnp.where(even, upper, lower)
            send_ref[y, z * half : (z + 1) * half, :] = jnp.where(even, lower, upper).astype(BF16)


def pack_kernel(
    all_sums, centered_ref, scaled_ref, centered_first, scaled_first, gated_ref, before_ref,
    scale_ref, keep_ref, sent_ref, gain_sum, value_in, gate_in,
    out_ref, conv_grad_ref, first_rows, value_ref, gate_ref, padded, sems,
    *, channels, taps_n, order,
):
    rows = gated_ref.shape[0]
    moved = ((value_in, value_ref), (gate_in, gate_ref))
    copies = [pltpu.make_async_copy(src, dst, sems.at[i]) for i, (src, dst) in enumerate(moved)]
    for c in copies:
        c.start()
    tile = all_sums[0]
    for j in range(1, all_sums.shape[0]):
        tile = tile + all_sums[j]
    tile = tile * (1.0 / channels)
    n_b = rows // LANES
    padded[0:HALO, :] = before_ref[...].astype(F32)
    padded[HALO : HALO + rows, :] = gated_ref[...].astype(F32)
    for b in range(n_b):
        at = b * LANES
        plain, cross = column(tile[b : b + 1]), column(tile[n_b + b : n_b + b + 1])
        scale = column(scale_ref[b : b + 1, :])
        centered, scaled = centered_ref[at : at + LANES, :], scaled_ref[at : at + LANES, :]
        if b == 0:
            centered = jnp.concatenate([centered_first[...], centered[HALO:]], axis=0)
            scaled = jnp.concatenate([scaled_first[...], scaled[HALO:]], axis=0)
        conv_grad_ref[at : at + LANES, :] = scale * (scaled - plain - centered * cross)
    first_rows[...] = conv_grad_ref[0:HALO, :]
    small = []
    for k0 in range(0, taps_n, 8):
        ks = range(k0, min(k0 + 8, taps_n))
        totals = {k: jnp.zeros((8, LANES), F32) for k in ks}
        for r in range(0, rows, 8):
            grad = conv_grad_ref[r : r + 8, :]
            for k in ks:
                totals[k] = totals[k] + grad * padded[2 + k + r : 10 + k + r, :]
        small += [jnp.sum(totals[k], axis=0, keepdims=True) for k in ks]
    small.append(jnp.sum(gain_sum[...], axis=0, keepdims=True))
    small = jnp.concatenate(small, axis=0).astype(BF16)
    big = keep_ref.shape[1]
    for j, y in enumerate(order):
        out_ref[j, 0:big, :] = (keep_ref[y] + sent_ref[y].astype(F32)).astype(BF16)
        out_ref[j, big : big + taps_n + 1, :] = small
    for c in copies:
        c.wait()


def middle_kernel(in_ref, out_ref, *, half, order):
    total = in_ref[0].astype(F32)
    for y in range(1, in_ref.shape[0]):
        total = total + in_ref[y].astype(F32)
    small = total[len(order) * half :].astype(BF16)
    for j, z in enumerate(order):
        out_ref[j, 0:half, :] = total[z * half : (z + 1) * half].astype(BF16)
        out_ref[j, half:, :] = small


def last_kernel(in_ref, weight_ref, taps_ref, gain_ref, *, order):
    half, taps_n = weight_ref.shape[0] // 2, taps_ref.shape[0]
    big, small = [None, None], None
    for j, z in enumerate(order):
        block = in_ref[j].astype(F32)
        own = big[z % 2]
        big[z % 2] = block[:half] if own is None else own + block[:half]
        small = block[half:] if small is None else small + block[half:]
    weight_ref[0:half, :] = big[0]
    weight_ref[half:, :] = big[1]
    taps_ref[...] = small[0:taps_n]
    gain_ref[...] = small[taps_n : taps_n + 1]


def glu_kernel(
    value_ref, gate_ref, conv_grad_ref, after_ref, taps, value_grad, gate_grad, padded
):
    rows, taps_n = value_ref.shape[0], taps.shape[0] - 1
    padded[0:rows, :] = conv_grad_ref[...]
    padded[rows : rows + HALO, :] = after_ref[...]
    for r in range(0, rows, BLOCK):
        gated_grad = weighted(taps, padded, r + taps_n - 1, BLOCK, -1)
        sig = jax.nn.sigmoid(gate_ref[r : r + BLOCK, :].astype(F32))
        value = value_ref[r : r + BLOCK, :].astype(F32)
        value_grad[r : r + BLOCK, :] = (gated_grad * sig).astype(BF16)
        gate_grad[r : r + BLOCK, :] = (gated_grad * value * sig * (1.0 - sig)).astype(BF16)


def passed_along(value, axis, by):
    length = lax.axis_size(axis)
    pairs = [(i, i + by) for i in range(length) if 0 <= i + by < length]
    return lax.ppermute(value, axis, pairs)


def listed(length, first):
    return tuple((first + i) % length for i in range(length))


def exchange(value, axis, order):
    return lax.all_to_all(
        value, axis, split_axis=0, concat_axis=0, tiled=True, axis_index_groups=[list(order)]
    )


def call(kernel, outs, in_specs, scratch=(), flops=0, final=False):
    run = pl.pallas_call(
        kernel,
        out_shape=[jax.ShapeDtypeStruct(*o) if final else pltpu.VMEM(*o) for o in outs],
        in_specs=in_specs,
        out_specs=[VMEM] * len(outs),
        scratch_shapes=list(scratch),
        cost_estimate=pl.CostEstimate(flops=flops, bytes_accessed=0, transcendentals=0),
        compiler_params=pltpu.CompilerParams(vmem_limit_bytes=16 << 20),
    )

    def with_operands(*operands):
        return run(
            *(
                pltpu.with_memory_space_constraint(x, spec.memory_space)
                for x, spec in zip(operands, in_specs)
            )
        )

    return with_operands


def per_device(
    glu_value, glu_gate, conv_taps, norm_gain, out_weight, norm_mean, norm_scale, out_grad
):
    rows, chans = glu_value.shape
    taps_n = conv_taps.shape[0]
    wide = out_grad.shape[1]
    n_z, n_y, n_tp = lax.axis_size("z"), lax.axis_size("y"), lax.axis_size("tp")
    own = wide // (n_z * n_y)
    half = own // 2
    order_z, order_y = listed(n_z, n_z * Z_FIRST // 16), listed(n_y, n_y * Y_FIRST // 8)
    order_tp = listed(n_tp, n_tp * TP_FIRST // 8)
    n_b = rows // LANES
    gain = norm_gain.reshape(1, chans)
    mean, scale = norm_mean.reshape(n_b, LANES), norm_scale.reshape(n_b, LANES)
    full, few = (rows, chans), (HALO, chans)

    (tail,) = call(
        tail_kernel, [(few, BF16)], [HBM, HBM],
        [pltpu.VMEM(few, BF16), pltpu.VMEM(few, BF16), pltpu.SemaphoreType.DMA((2,))],
        flops=1 << 30,
    )(glu_value, glu_gate)
    before = passed_along(tail, SP, 1)
    (taps, gated, centered, scaled, activated, conv0, act0, gain_sum, sums) = call(
        main_kernel,
        [((taps_n + 1, chans), F32), (full, BF16), (full, F32), (full, F32), (full, BF16),
         (few, F32), (few, F32), ((8, chans), F32), ((2 * n_b, LANES), F32)],
        [VMEM] * 8,
        [pltpu.VMEM((HALO + rows, chans), F32), pltpu.VMEM(full, F32)],
        flops=1 << 28,
    )(glu_value, glu_gate, conv_taps, gain, mean, scale, out_weight, out_grad)
    centered0, scaled0, activated0, gain_sum, sums = call(
        first_kernel,
        [(few, F32), (few, F32), (few, BF16), ((8, chans), F32), ((n_tp, 2 * n_b, LANES), F32)],
        [VMEM] * 9,
        [pltpu.VMEM((2 * HALO, chans), F32)],
        flops=1 << 24,
    )(before, conv0, act0, taps, gain, mean, scale, gain_sum, sums)
    keep, send = call(
        functools.partial(weight_kernel, n_z=n_z, n_y=n_y),
        [((n_y, n_z * half, chans), F32), ((n_y, n_z * half, chans), BF16)],
        [VMEM] * 3, flops=1 << 28,
    )(out_grad, activated, activated0)
    sent = lax.ppermute(send, "z", [(i, i ^ 1) for i in range(n_z)])
    sums = exchange(sums, "tp", order_tp)
    packed, conv_grad, first_rows, value, gate = call(
        functools.partial(pack_kernel, channels=chans * n_tp, taps_n=taps_n, order=order_y),
        [((n_y, n_z * half + taps_n + 1, chans), BF16), (full, F32), (few, F32), (full, BF16),
         (full, BF16)],
        [VMEM] * 11 + [HBM] * 2,
        [pltpu.VMEM((HALO + rows, chans), F32), pltpu.SemaphoreType.DMA((2,))],
        flops=1 << 26,
    )(sums, centered, scaled, centered0, scaled0, gated, before, scale, keep, sent, gain_sum,
      glu_value, glu_gate)
    packed = exchange(packed, "y", order_y)
    (packed,) = call(
        functools.partial(middle_kernel, half=half, order=order_z),
        [((n_z, half + taps_n + 1, chans), BF16)], [VMEM], flops=1 << 22,
    )(packed)
    packed = exchange(packed, "z", order_z)
    after = passed_along(first_rows, SP, -1)
    value_grad, gate_grad = call(
        glu_kernel, [(full, BF16), (full, BF16)], [VMEM] * 5,
        [pltpu.VMEM((rows + HALO, chans), F32)], flops=1 << 28, final=True,
    )(value, gate, conv_grad, after, taps)
    weight_grad, taps_grad, gain_grad = call(
        functools.partial(last_kernel, order=order_z),
        [((own, chans), F32), ((taps_n, chans), F32), ((1, chans), F32)], [VMEM], flops=1 << 22,
        final=True,
    )(packed)
    return (value_grad, gate_grad, taps_grad, gain_grad.reshape(chans), weight_grad)


def solution(mesh):
    shape = (16, 8) if mesh.shape["sp"] == 128 else (mesh.shape["sp"] // 2, 2)
    torus = Mesh(mesh.devices.reshape(*shape, mesh.shape["tp"]), ("z", "y", "tp"))
    placed = (
        P(SP, "tp"),
        P(SP, "tp"),
        P(None, "tp"),
        P("tp"),
        P(None, "tp"),
        P(SP),
        P(SP),
        P(SP, None),
    )

    return jax.shard_map(
        per_device,
        mesh=torus,
        in_specs=placed,
        out_specs=(P(SP, "tp"), P(SP, "tp"), P(None, "tp"), P("tp"), P(SP, "tp")),
        check_vma=False,
    )
```

```python
import functools

import jax
import jax.numpy as jnp
from jax import lax
from jax.experimental import pallas as pl
from jax.experimental.pallas import tpu as pltpu
from jax.sharding import Mesh
from jax.sharding import PartitionSpec as P

SP = ("z", "y")
HALO = 32
BLOCK = 64
LANES = 128
Z_FIRST, Y_FIRST, TP_FIRST = 12, 5, 5
F32, BF16 = jnp.float32, jnp.bfloat16
VMEM = pl.BlockSpec(memory_space=pltpu.VMEM)
HBM = pl.BlockSpec(memory_space=pltpu.HBM)


def column(row):
    return jnp.transpose(jnp.broadcast_to(row, (LANES, LANES)))


def row_sums(block):
    return jnp.sum(jnp.transpose(block), axis=0, keepdims=True)


def weighted(taps_ref, source_ref, first, rows, step):
    total = None
    for k in range(taps_ref.shape[0] - 1):
        begin = first + step * k
        term = taps_ref[k : k + 1, :] * source_ref[begin : begin + rows, :]
        total = term if total is None else total + term
    return total


def silu_parts(conv, mean, scale, gain, act_grad):
    centered = (conv - mean) * scale
    normed = centered * gain
    sig = jax.nn.sigmoid(normed)
    normed_grad = act_grad * sig * (1.0 + normed * (1.0 - sig))
    return centered, (normed * sig).astype(BF16), normed_grad, normed_grad * gain


def tail_kernel(value_ref, gate_ref, out_ref, value_rows, gate_rows, sems):
    first = value_ref.shape[0] - HALO
    copies = [
        pltpu.make_async_copy(ref.at[pl.ds(first, HALO)], rows, sems.at[i])
        for i, (ref, rows) in enumerate(((value_ref, value_rows), (gate_ref, gate_rows)))
    ]
    for c in copies:
        c.start()
    for c in copies:
        c.wait()
    sig = jax.nn.sigmoid(gate_rows[...].astype(F32))
    out_ref[...] = (value_rows[...].astype(F32) * sig).astype(BF16)


def main_kernel(
    value_ref, gate_ref, taps_raw, gain_ref, mean_ref, scale_ref, weight_ref, out_grad_ref,
    taps, gated_ref, centered_ref, scaled_ref, activated_ref, conv_first, act_first, gain_sum,
    sums_ref, padded, conv_ref,
):
    rows, taps_n = value_ref.shape[0], taps_raw.shape[0]
    taps[0:taps_n, :] = taps_raw[...].astype(F32)
    gated = (value_ref[...].astype(F32) * jax.nn.sigmoid(gate_ref[...].astype(F32))).astype(BF16)
    gated_ref[...] = gated
    padded[0:HALO, :] = jnp.zeros((HALO, LANES), F32)
    padded[HALO : HALO + rows, :] = gated.astype(F32)
    for r in range(0, rows, BLOCK):
        conv_ref[r : r + BLOCK, :] = weighted(taps, padded, 2 + r, BLOCK, 1)
    conv_first[...] = conv_ref[0:HALO, :]
    gain = gain_ref[...]
    gain_total = jnp.zeros((8, LANES), F32)
    n_b = rows // LANES
    for b in range(n_b):
        at = b * LANES
        mean, scale = column(mean_ref[b : b + 1, :]), column(scale_ref[b : b + 1, :])
        act_grad = jnp.dot(
            out_grad_ref[at : at + LANES, :], weight_ref[...], preferred_element_type=F32
        )
        if b == 0:
            act_first[...] = act_grad[:HALO]
        plain, cross = [], []
        for h in range(0, LANES, BLOCK):
            r = at + h
            centered, activated, normed_grad, scaled = silu_parts(
                conv_ref[r : r + BLOCK, :], mean[h : h + BLOCK], scale[h : h + BLOCK], gain,
                act_grad[h : h + BLOCK],
            )
            centered_ref[r : r + BLOCK, :] = centered
            scaled_ref[r : r + BLOCK, :] = scaled
            activated_ref[r : r + BLOCK, :] = activated
            for_gain = normed_grad * centered
            if r == 0:
                for_gain = for_gain[HALO:]
            gain_total += jnp.sum(for_gain.reshape(-1, 8, LANES), axis=0)
            plain.append(scaled)
            cross.append(scaled * centered)
        sums_ref[b : b + 1, :] = row_sums(jnp.concatenate(plain, axis=0))
        sums_ref[n_b + b : n_b + b + 1, :] = row_sums(jnp.concatenate(cross, axis=0))
    gain_sum[...] = gain_total


def first_kernel(
    before_ref, conv_first, act_first, taps, gain_ref, mean_ref, scale_ref, gain_sum, sums_ref,
    centered_ref, scaled_ref, activated_ref, gain_out, sums_out,
    padded,
):
    padded[0:HALO, :] = before_ref[...].astype(F32)
    padded[HALO : 2 * HALO, :] = jnp.zeros((HALO, LANES), F32)
    conv = conv_first[...] + weighted(taps, padded, 2, HALO, 1)
    mean, scale = column(mean_ref[0:1, :])[:HALO], column(scale_ref[0:1, :])[:HALO]
    centered, activated, normed_grad, scaled = silu_parts(
        conv, mean, scale, gain_ref[...], act_first[...]
    )
    centered_ref[...] = centered
    scaled_ref[...] = scaled
    activated_ref[...] = activated
    gain_out[...] = gain_sum[...] + jnp.sum((normed_grad * centered).reshape(-1, 8, LANES), axis=0)
    filler = jnp.zeros((LANES - HALO, LANES), F32)
    plain = row_sums(jnp.concatenate([scaled, filler], axis=0))
    cross = row_sums(jnp.concatenate([scaled * centered, filler], axis=0))
    tile = sums_ref[...]
    n_b = tile.shape[0] // 2
    at_row = lax.broadcasted_iota(jnp.int32, tile.shape, 0)
    mine = lax.broadcasted_iota(jnp.int32, tile.shape, 1) < HALO
    tile = jnp.where((at_row == 0) & mine, plain, tile)
    tile = jnp.where((at_row == n_b) & mine, cross, tile)
    for j in range(sums_out.shape[0]):
        sums_out[j] = tile


def weight_kernel(
    out_grad_ref, activated_ref, activated_first, keep_ref, send_ref, *, n_z, n_y
):
    activated = jnp.concatenate([activated_first[...], activated_ref[HALO:, :]], axis=0)
    part = lax.dot_general(
        out_grad_ref[...], activated, (((0,), (0,)), ((), ())), preferred_element_type=F32
    )
    own = part.shape[0] // (n_z * n_y)
    half = own // 2
    even = jnp.full((half, part.shape[1]), lax.axis_index("z") & 1, jnp.int32) == 0
    for z in range(n_z):
        for y in range(n_y):
            at = (z * n_y + y) * own
            upper, lower = part[at : at + half], part[at + half : at + own]
            keep_ref[y, z * half : (z + 1) * half, :] = jnp.where(even, upper, lower)
            send_ref[y, z * half : (z + 1) * half, :] = jnp.where(even, lower, upper).astype(BF16)


def pack_kernel(
    all_sums, centered_ref, scaled_ref, centered_first, scaled_first, gated_ref, before_ref,
    scale_ref, keep_ref, sent_ref, gain_sum, value_in, gate_in,
    out_ref, conv_grad_ref, first_rows, value_ref, gate_ref, padded, sems,
    *, channels, taps_n, order,
):
    rows = gated_ref.shape[0]
    moved = ((value_in, value_ref), (gate_in, gate_ref))
    copies = [pltpu.make_async_copy(src, dst, sems.at[i]) for i, (src, dst) in enumerate(moved)]
    for c in copies:
        c.start()
    tile = all_sums[0]
    for j in range(1, all_sums.shape[0]):
        tile = tile + all_sums[j]
    tile = tile * (1.0 / channels)
    n_b = rows // LANES
    padded[0:HALO, :] = before_ref[...].astype(F32)
    padded[HALO : HALO + rows, :] = gated_ref[...].astype(F32)
    for b in range(n_b):
        at = b * LANES
        plain, cross = column(tile[b : b + 1]), column(tile[n_b + b : n_b + b + 1])
        scale = column(scale_ref[b : b + 1, :])
        centered, scaled = centered_ref[at : at + LANES, :], scaled_ref[at : at + LANES, :]
        if b == 0:
            centered = jnp.concatenate([centered_first[...], centered[HALO:]], axis=0)
            scaled = jnp.concatenate([scaled_first[...], scaled[HALO:]], axis=0)
        conv_grad_ref[at : at + LANES, :] = scale * (scaled - plain - centered * cross)
    first_rows[...] = conv_grad_ref[0:HALO, :]
    small = []
    for k0 in range(0, taps_n, 8):
        ks = range(k0, min(k0 + 8, taps_n))
        totals = {k: jnp.zeros((8, LANES), F32) for k in ks}
        for r in range(0, rows, 8):
            grad = conv_grad_ref[r : r + 8, :]
            for k in ks:
                totals[k] = totals[k] + grad * padded[2 + k + r : 10 + k + r, :]
        small += [jnp.sum(totals[k], axis=0, keepdims=True) for k in ks]
    small.append(jnp.sum(gain_sum[...], axis=0, keepdims=True))
    small = jnp.concatenate(small, axis=0).astype(BF16)
    big = keep_ref.shape[1]
    for j, y in enumerate(order):
        out_ref[j, 0:big, :] = (keep_ref[y] + sent_ref[y].astype(F32)).astype(BF16)
        out_ref[j, big : big + taps_n + 1, :] = small
    for c in copies:
        c.wait()


def middle_kernel(in_ref, out_ref, *, half, order):
    total = in_ref[0].astype(F32)
    for y in range(1, in_ref.shape[0]):
        total = total + in_ref[y].astype(F32)
    small = total[len(order) * half :].astype(BF16)
    for j, z in enumerate(order):
        out_ref[j, 0:half, :] = total[z * half : (z + 1) * half].astype(BF16)
        out_ref[j, half:, :] = small


def last_kernel(in_ref, weight_ref, taps_ref, gain_ref, *, order):
    half, taps_n = weight_ref.shape[0] // 2, taps_ref.shape[0]
    big, small = [None, None], None
    for j, z in enumerate(order):
        block = in_ref[j].astype(F32)
        own = big[z % 2]
        big[z % 2] = block[:half] if own is None else own + block[:half]
        small = block[half:] if small is None else small + block[half:]
    weight_ref[0:half, :] = big[0]
    weight_ref[half:, :] = big[1]
    taps_ref[...] = small[0:taps_n]
    gain_ref[...] = small[taps_n : taps_n + 1]


def glu_block(value_ref, gate_ref, taps, padded, at, first, rows):
    gated_grad = weighted(taps, padded, first + taps.shape[0] - 2, rows, -1)
    sig = jax.nn.sigmoid(gate_ref[at : at + rows, :].astype(F32))
    value = value_ref[at : at + rows, :].astype(F32)
    return (gated_grad * sig).astype(BF16), (gated_grad * value * sig * (1.0 - sig)).astype(BF16)


def glu_kernel(value_ref, gate_ref, conv_grad_ref, taps, value_out, gate_out, value_grad, gate_grad, sems):
    rows = value_ref.shape[0] - HALO
    copies = [
        pltpu.make_async_copy(src.at[pl.ds(0, rows)], dst.at[pl.ds(0, rows)], sems.at[i])
        for i, (src, dst) in enumerate(((value_grad, value_out), (gate_grad, gate_out)))
    ]
    for r in range(0, rows, BLOCK):
        n = min(BLOCK, rows - r)
        value_grad[r : r + n, :], gate_grad[r : r + n, :] = glu_block(
            value_ref, gate_ref, taps, conv_grad_ref, r, r, n
        )
    for c in copies:
        c.start()
    for c in copies:
        c.wait()


def glu_end_kernel(
    value_ref, gate_ref, conv_grad_ref, after_ref, taps, value_in, gate_in, value_out, gate_out,
    padded, value_grad, gate_grad, sems,
):
    rows = value_ref.shape[0] - HALO
    copies = [
        pltpu.make_async_copy(src, dst.at[pl.ds(rows, HALO)], sems.at[i])
        for i, (src, dst) in enumerate(((value_grad, value_out), (gate_grad, gate_out)))
    ]
    padded[0:HALO, :] = conv_grad_ref[rows:, :]
    padded[HALO:, :] = after_ref[...]
    value_grad[...], gate_grad[...] = glu_block(value_ref, gate_ref, taps, padded, rows, 0, HALO)
    for c in copies:
        c.start()
    for c in copies:
        c.wait()


def passed_along(value, axis, by):
    length = lax.axis_size(axis)
    pairs = [(i, i + by) for i in range(length) if 0 <= i + by < length]
    return lax.ppermute(value, axis, pairs)


def listed(length, first):
    return tuple((first + i) % length for i in range(length))


def exchange(value, axis, order):
    return lax.all_to_all(
        value, axis, split_axis=0, concat_axis=0, tiled=True, axis_index_groups=[list(order)]
    )


def call(kernel, outs, in_specs, scratch=(), flops=0, final=False, out_spec=VMEM, aliases=None):
    run = pl.pallas_call(
        kernel,
        out_shape=[jax.ShapeDtypeStruct(*o) if final else pltpu.VMEM(*o) for o in outs],
        in_specs=in_specs,
        out_specs=[out_spec] * len(outs),
        input_output_aliases=aliases or {},
        scratch_shapes=list(scratch),
        cost_estimate=pl.CostEstimate(flops=flops, bytes_accessed=0, transcendentals=0),
        compiler_params=pltpu.CompilerParams(vmem_limit_bytes=16 << 20),
    )

    def with_operands(*operands):
        return run(
            *(
                pltpu.with_memory_space_constraint(x, spec.memory_space)
                for x, spec in zip(operands, in_specs)
            )
        )

    return with_operands


def per_device(
    glu_value, glu_gate, conv_taps, norm_gain, out_weight, norm_mean, norm_scale, out_grad
):
    rows, chans = glu_value.shape
    taps_n = conv_taps.shape[0]
    wide = out_grad.shape[1]
    n_z, n_y, n_tp = lax.axis_size("z"), lax.axis_size("y"), lax.axis_size("tp")
    own = wide // (n_z * n_y)
    half = own // 2
    order_z, order_y = listed(n_z, n_z * Z_FIRST // 16), listed(n_y, n_y * Y_FIRST // 8)
    order_tp = listed(n_tp, n_tp * TP_FIRST // 8)
    n_b = rows // LANES
    gain = norm_gain.reshape(1, chans)
    mean, scale = norm_mean.reshape(n_b, LANES), norm_scale.reshape(n_b, LANES)
    full, few = (rows, chans), (HALO, chans)

    (tail,) = call(
        tail_kernel, [(few, BF16)], [HBM, HBM],
        [pltpu.VMEM(few, BF16), pltpu.VMEM(few, BF16), pltpu.SemaphoreType.DMA((2,))],
        flops=1 << 30,
    )(glu_value, glu_gate)
    before = passed_along(tail, SP, 1)
    (taps, gated, centered, scaled, activated, conv0, act0, gain_sum, sums) = call(
        main_kernel,
        [((taps_n + 1, chans), F32), (full, BF16), (full, F32), (full, F32), (full, BF16),
         (few, F32), (few, F32), ((8, chans), F32), ((2 * n_b, LANES), F32)],
        [VMEM] * 8,
        [pltpu.VMEM((HALO + rows, chans), F32), pltpu.VMEM(full, F32)],
        flops=1 << 28,
    )(glu_value, glu_gate, conv_taps, gain, mean, scale, out_weight, out_grad)
    centered0, scaled0, activated0, gain_sum, sums = call(
        first_kernel,
        [(few, F32), (few, F32), (few, BF16), ((8, chans), F32), ((n_tp, 2 * n_b, LANES), F32)],
        [VMEM] * 9,
        [pltpu.VMEM((2 * HALO, chans), F32)],
        flops=1 << 24,
    )(before, conv0, act0, taps, gain, mean, scale, gain_sum, sums)
    keep, send = call(
        functools.partial(weight_kernel, n_z=n_z, n_y=n_y),
        [((n_y, n_z * half, chans), F32), ((n_y, n_z * half, chans), BF16)],
        [VMEM] * 3, flops=1 << 28,
    )(out_grad, activated, activated0)
    sent = lax.ppermute(send, "z", [(i, i ^ 1) for i in range(n_z)])
    sums = exchange(sums, "tp", order_tp)
    packed, conv_grad, first_rows, value, gate = call(
        functools.partial(pack_kernel, channels=chans * n_tp, taps_n=taps_n, order=order_y),
        [((n_y, n_z * half + taps_n + 1, chans), BF16), (full, F32), (few, F32), (full, BF16),
         (full, BF16)],
        [VMEM] * 11 + [HBM] * 2,
        [pltpu.VMEM((HALO + rows, chans), F32), pltpu.SemaphoreType.DMA((2,))],
        flops=1 << 26,
    )(sums, centered, scaled, centered0, scaled0, gated, before, scale, keep, sent, gain_sum,
      glu_value, glu_gate)
    packed = exchange(packed, "y", order_y)
    (packed,) = call(
        functools.partial(middle_kernel, half=half, order=order_z),
        [((n_z, half + taps_n + 1, chans), BF16)], [VMEM], flops=1 << 22,
    )(packed)
    packed = exchange(packed, "z", order_z)
    after = passed_along(first_rows, SP, -1)
    value_grad, gate_grad = call(
        glu_kernel, [(full, BF16), (full, BF16)], [VMEM] * 4,
        [pltpu.VMEM(full, BF16), pltpu.VMEM(full, BF16), pltpu.SemaphoreType.DMA((2,))],
        flops=1 << 28, final=True, out_spec=HBM,
    )(value, gate, conv_grad, taps)
    value_grad, gate_grad = call(
        glu_end_kernel, [(full, BF16), (full, BF16)], [VMEM] * 5 + [HBM] * 2,
        [pltpu.VMEM((2 * HALO, chans), F32), pltpu.VMEM(few, BF16), pltpu.VMEM(few, BF16),
         pltpu.SemaphoreType.DMA((2,))],
        flops=1 << 24, final=True, out_spec=HBM, aliases={5: 0, 6: 1},
    )(value, gate, conv_grad, after, taps, value_grad, gate_grad)
    weight_grad, taps_grad, gain_grad = call(
        functools.partial(last_kernel, order=order_z),
        [((own, chans), F32), ((taps_n, chans), F32), ((1, chans), F32)], [VMEM], flops=1 << 22,
        final=True,
    )(packed)
    return (value_grad, gate_grad, taps_grad, gain_grad.reshape(chans), weight_grad)


def solution(mesh):
    shape = (16, 8) if mesh.shape["sp"] == 128 else (mesh.shape["sp"] // 2, 2)
    torus = Mesh(mesh.devices.reshape(*shape, mesh.shape["tp"]), ("z", "y", "tp"))
    placed = (
        P(SP, "tp"),
        P(SP, "tp"),
        P(None, "tp"),
        P("tp"),
        P(None, "tp"),
        P(SP),
        P(SP),
        P(SP, None),
    )

    return jax.shard_map(
        per_device,
        mesh=torus,
        in_specs=placed,
        out_specs=(P(SP, "tp"), P(SP, "tp"), P(None, "tp"), P("tp"), P(SP, "tp")),
        check_vma=False,
    )
```

```python
import functools

import jax
import jax.numpy as jnp
from jax import lax
from jax.experimental import pallas as pl
from jax.experimental.pallas import tpu as pltpu
from jax.sharding import Mesh
from jax.sharding import PartitionSpec as P

SP = ("z", "y")
HALO = 32
BLOCK = 64
LANES = 128
Z_FIRST, Y_FIRST, TP_FIRST = 12, 5, 5
F32, BF16 = jnp.float32, jnp.bfloat16
VMEM = pl.BlockSpec(memory_space=pltpu.VMEM)
HBM = pl.BlockSpec(memory_space=pltpu.HBM)


def column(row):
    return jnp.transpose(jnp.broadcast_to(row, (LANES, LANES)))


def row_sums(block):
    return jnp.sum(jnp.transpose(block), axis=0, keepdims=True)


def weighted(taps_ref, source_ref, first, rows, step):
    total = None
    for k in range(taps_ref.shape[0] - 1):
        begin = first + step * k
        term = taps_ref[k : k + 1, :] * source_ref[begin : begin + rows, :]
        total = term if total is None else total + term
    return total


def silu_parts(conv, mean, scale, gain, act_grad):
    centered = (conv - mean) * scale
    normed = centered * gain
    sig = jax.nn.sigmoid(normed)
    normed_grad = act_grad * sig * (1.0 + normed * (1.0 - sig))
    return centered, (normed * sig).astype(BF16), normed_grad, normed_grad * gain


def tail_kernel(value_ref, gate_ref, out_ref, value_rows, gate_rows, sems):
    first = value_ref.shape[0] - HALO
    copies = [
        pltpu.make_async_copy(ref.at[pl.ds(first, HALO)], rows, sems.at[i])
        for i, (ref, rows) in enumerate(((value_ref, value_rows), (gate_ref, gate_rows)))
    ]
    for c in copies:
        c.start()
    for c in copies:
        c.wait()
    sig = jax.nn.sigmoid(gate_rows[...].astype(F32))
    out_ref[...] = (value_rows[...].astype(F32) * sig).astype(BF16)


def main_kernel(
    value_ref, gate_ref, taps_raw, gain_ref, mean_ref, scale_ref, weight_ref, out_grad_ref,
    taps, gated_ref, centered_ref, scaled_ref, activated_ref, conv_first, act_first, gain_sum,
    sums_ref, padded, conv_ref,
):
    rows, taps_n = value_ref.shape[0], taps_raw.shape[0]
    taps[0:taps_n, :] = taps_raw[...].astype(F32)
    gated = (value_ref[...].astype(F32) * jax.nn.sigmoid(gate_ref[...].astype(F32))).astype(BF16)
    gated_ref[...] = gated
    padded[0:HALO, :] = jnp.zeros((HALO, LANES), F32)
    padded[HALO : HALO + rows, :] = gated.astype(F32)
    for r in range(0, rows, BLOCK):
        conv_ref[r : r + BLOCK, :] = weighted(taps, padded, 2 + r, BLOCK, 1)
    conv_first[...] = conv_ref[0:HALO, :]
    gain = gain_ref[...]
    gain_total = jnp.zeros((8, LANES), F32)
    n_b = rows // LANES
    for b in range(n_b):
        at = b * LANES
        mean, scale = column(mean_ref[b : b + 1, :]), column(scale_ref[b : b + 1, :])
        act_grad = jnp.dot(
            out_grad_ref[at : at + LANES, :], weight_ref[...], preferred_element_type=F32
        )
        if b == 0:
            act_first[...] = act_grad[:HALO]
        plain, cross = [], []
        for h in range(0, LANES, BLOCK):
            r = at + h
            centered, activated, normed_grad, scaled = silu_parts(
                conv_ref[r : r + BLOCK, :], mean[h : h + BLOCK], scale[h : h + BLOCK], gain,
                act_grad[h : h + BLOCK],
            )
            centered_ref[r : r + BLOCK, :] = centered
            scaled_ref[r : r + BLOCK, :] = scaled
            activated_ref[r : r + BLOCK, :] = activated
            for_gain = normed_grad * centered
            if r == 0:
                for_gain = for_gain[HALO:]
            gain_total += jnp.sum(for_gain.reshape(-1, 8, LANES), axis=0)
            plain.append(scaled)
            cross.append(scaled * centered)
        sums_ref[b : b + 1, :] = row_sums(jnp.concatenate(plain, axis=0))
        sums_ref[n_b + b : n_b + b + 1, :] = row_sums(jnp.concatenate(cross, axis=0))
    gain_sum[...] = gain_total


def first_kernel(
    before_ref, conv_first, act_first, taps, gain_ref, mean_ref, scale_ref, gain_sum, sums_ref,
    centered_ref, scaled_ref, activated_ref, gain_out, sums_out,
    padded,
):
    padded[0:HALO, :] = before_ref[...].astype(F32)
    padded[HALO : 2 * HALO, :] = jnp.zeros((HALO, LANES), F32)
    conv = conv_first[...] + weighted(taps, padded, 2, HALO, 1)
    mean, scale = column(mean_ref[0:1, :])[:HALO], column(scale_ref[0:1, :])[:HALO]
    centered, activated, normed_grad, scaled = silu_parts(
        conv, mean, scale, gain_ref[...], act_first[...]
    )
    centered_ref[...] = centered
    scaled_ref[...] = scaled
    activated_ref[...] = activated
    gain_out[...] = gain_sum[...] + jnp.sum((normed_grad * centered).reshape(-1, 8, LANES), axis=0)
    filler = jnp.zeros((LANES - HALO, LANES), F32)
    plain = row_sums(jnp.concatenate([scaled, filler], axis=0))
    cross = row_sums(jnp.concatenate([scaled * centered, filler], axis=0))
    tile = sums_ref[...]
    n_b = tile.shape[0] // 2
    at_row = lax.broadcasted_iota(jnp.int32, tile.shape, 0)
    mine = lax.broadcasted_iota(jnp.int32, tile.shape, 1) < HALO
    tile = jnp.where((at_row == 0) & mine, plain, tile)
    tile = jnp.where((at_row == n_b) & mine, cross, tile)
    for j in range(sums_out.shape[0]):
        sums_out[j] = tile


def weight_kernel(
    out_grad_ref, activated_ref, activated_first, keep_ref, send_ref, *, n_z, n_y
):
    activated = jnp.concatenate([activated_first[...], activated_ref[HALO:, :]], axis=0)
    part = lax.dot_general(
        out_grad_ref[...], activated, (((0,), (0,)), ((), ())), preferred_element_type=F32
    )
    own = part.shape[0] // (n_z * n_y)
    half = own // 2
    even = jnp.full((half, part.shape[1]), lax.axis_index("z") & 1, jnp.int32) == 0
    for z in range(n_z):
        for y in range(n_y):
            at = (z * n_y + y) * own
            upper, lower = part[at : at + half], part[at + half : at + own]
            keep_ref[y, z * half : (z + 1) * half, :] = jnp.where(even, upper, lower)
            send_ref[y, z * half : (z + 1) * half, :] = jnp.where(even, lower, upper).astype(BF16)


def first_weight_kernel(
    before_ref, conv_first, act_first, taps, gain_ref, mean_ref, scale_ref, gain_sum, sums_ref,
    out_grad_ref, activated_ref,
    centered_first, scaled_first, gain_out, sums_out, keep_ref, send_ref,
    padded, activated_first,
    *, n_z, n_y,
):
    first_kernel(
        before_ref, conv_first, act_first, taps, gain_ref, mean_ref, scale_ref, gain_sum, sums_ref,
        centered_first, scaled_first, activated_first, gain_out, sums_out, padded,
    )
    weight_kernel(
        out_grad_ref, activated_ref, activated_first, keep_ref, send_ref, n_z=n_z, n_y=n_y
    )


def pack_kernel(
    all_sums, centered_ref, scaled_ref, centered_first, scaled_first, gated_ref, before_ref,
    scale_ref, keep_ref, sent_ref, gain_sum, value_in, gate_in,
    out_ref, conv_grad_ref, first_rows, value_ref, gate_ref, padded, sems,
    *, channels, taps_n, order,
):
    rows = gated_ref.shape[0]
    moved = ((value_in, value_ref), (gate_in, gate_ref))
    copies = [pltpu.make_async_copy(src, dst, sems.at[i]) for i, (src, dst) in enumerate(moved)]
    for c in copies:
        c.start()
    tile = all_sums[0]
    for j in range(1, all_sums.shape[0]):
        tile = tile + all_sums[j]
    tile = tile * (1.0 / channels)
    n_b = rows // LANES
    padded[0:HALO, :] = before_ref[...].astype(F32)
    padded[HALO : HALO + rows, :] = gated_ref[...].astype(F32)
    for b in range(n_b):
        at = b * LANES
        plain, cross = column(tile[b : b + 1]), column(tile[n_b + b : n_b + b + 1])
        scale = column(scale_ref[b : b + 1, :])
        centered, scaled = centered_ref[at : at + LANES, :], scaled_ref[at : at + LANES, :]
        if b == 0:
            centered = jnp.concatenate([centered_first[...], centered[HALO:]], axis=0)
            scaled = jnp.concatenate([scaled_first[...], scaled[HALO:]], axis=0)
        conv_grad_ref[at : at + LANES, :] = scale * (scaled - plain - centered * cross)
    first_rows[...] = conv_grad_ref[0:HALO, :]
    small = []
    for k0 in range(0, taps_n, 8):
        ks = range(k0, min(k0 + 8, taps_n))
        totals = {k: jnp.zeros((8, LANES), F32) for k in ks}
        for r in range(0, rows, 8):
            grad = conv_grad_ref[r : r + 8, :]
            for k in ks:
                totals[k] = totals[k] + grad * padded[2 + k + r : 10 + k + r, :]
        small += [jnp.sum(totals[k], axis=0, keepdims=True) for k in ks]
    small.append(jnp.sum(gain_sum[...], axis=0, keepdims=True))
    small = jnp.concatenate(small, axis=0).astype(BF16)
    big = keep_ref.shape[1]
    for j, y in enumerate(order):
        out_ref[j, 0:big, :] = (keep_ref[y] + sent_ref[y].astype(F32)).astype(BF16)
        out_ref[j, big : big + taps_n + 1, :] = small
    for c in copies:
        c.wait()


def middle_kernel(in_ref, out_ref, *, half, order):
    total = in_ref[0].astype(F32)
    for y in range(1, in_ref.shape[0]):
        total = total + in_ref[y].astype(F32)
    small = total[len(order) * half :].astype(BF16)
    for j, z in enumerate(order):
        out_ref[j, 0:half, :] = total[z * half : (z + 1) * half].astype(BF16)
        out_ref[j, half:, :] = small


def last_kernel(in_ref, weight_ref, taps_ref, gain_ref, *, order):
    half, taps_n = weight_ref.shape[0] // 2, taps_ref.shape[0]
    big, small = [None, None], None
    for j, z in enumerate(order):
        block = in_ref[j].astype(F32)
        own = big[z % 2]
        big[z % 2] = block[:half] if own is None else own + block[:half]
        small = block[half:] if small is None else small + block[half:]
    weight_ref[0:half, :] = big[0]
    weight_ref[half:, :] = big[1]
    taps_ref[...] = small[0:taps_n]
    gain_ref[...] = small[taps_n : taps_n + 1]


def glu_block(value_ref, gate_ref, taps, padded, at, first, rows):
    gated_grad = weighted(taps, padded, first + taps.shape[0] - 2, rows, -1)
    sig = jax.nn.sigmoid(gate_ref[at : at + rows, :].astype(F32))
    value = value_ref[at : at + rows, :].astype(F32)
    return (gated_grad * sig).astype(BF16), (gated_grad * value * sig * (1.0 - sig)).astype(BF16)


def glu_kernel(value_ref, gate_ref, conv_grad_ref, taps, value_out, gate_out, value_grad, gate_grad, sems):
    rows = value_ref.shape[0] - HALO
    copies = [
        pltpu.make_async_copy(src.at[pl.ds(0, rows)], dst.at[pl.ds(0, rows)], sems.at[i])
        for i, (src, dst) in enumerate(((value_grad, value_out), (gate_grad, gate_out)))
    ]
    for r in range(0, rows, BLOCK):
        n = min(BLOCK, rows - r)
        value_grad[r : r + n, :], gate_grad[r : r + n, :] = glu_block(
            value_ref, gate_ref, taps, conv_grad_ref, r, r, n
        )
    for c in copies:
        c.start()
    for c in copies:
        c.wait()


def glu_end_kernel(
    value_ref, gate_ref, conv_grad_ref, after_ref, taps, value_in, gate_in, value_out, gate_out,
    padded, value_grad, gate_grad, sems,
):
    rows = value_ref.shape[0] - HALO
    copies = [
        pltpu.make_async_copy(src, dst.at[pl.ds(rows, HALO)], sems.at[i])
        for i, (src, dst) in enumerate(((value_grad, value_out), (gate_grad, gate_out)))
    ]
    padded[0:HALO, :] = conv_grad_ref[rows:, :]
    padded[HALO:, :] = after_ref[...]
    value_grad[...], gate_grad[...] = glu_block(value_ref, gate_ref, taps, padded, rows, 0, HALO)
    for c in copies:
        c.start()
    for c in copies:
        c.wait()


def passed_along(value, axis, by):
    length = lax.axis_size(axis)
    pairs = [(i, i + by) for i in range(length) if 0 <= i + by < length]
    return lax.ppermute(value, axis, pairs)


def listed(length, first):
    return tuple((first + i) % length for i in range(length))


def exchange(value, axis, order):
    return lax.all_to_all(
        value, axis, split_axis=0, concat_axis=0, tiled=True, axis_index_groups=[list(order)]
    )


def call(kernel, outs, in_specs, scratch=(), flops=0, final=False, out_spec=VMEM, aliases=None):
    run = pl.pallas_call(
        kernel,
        out_shape=[jax.ShapeDtypeStruct(*o) if final else pltpu.VMEM(*o) for o in outs],
        in_specs=in_specs,
        out_specs=[out_spec] * len(outs),
        input_output_aliases=aliases or {},
        scratch_shapes=list(scratch),
        cost_estimate=pl.CostEstimate(flops=flops, bytes_accessed=0, transcendentals=0),
        compiler_params=pltpu.CompilerParams(vmem_limit_bytes=16 << 20),
    )

    def with_operands(*operands):
        return run(
            *(
                pltpu.with_memory_space_constraint(x, spec.memory_space)
                for x, spec in zip(operands, in_specs)
            )
        )

    return with_operands


def per_device(
    glu_value, glu_gate, conv_taps, norm_gain, out_weight, norm_mean, norm_scale, out_grad
):
    rows, chans = glu_value.shape
    taps_n = conv_taps.shape[0]
    wide = out_grad.shape[1]
    n_z, n_y, n_tp = lax.axis_size("z"), lax.axis_size("y"), lax.axis_size("tp")
    own = wide // (n_z * n_y)
    half = own // 2
    order_z, order_y = listed(n_z, n_z * Z_FIRST // 16), listed(n_y, n_y * Y_FIRST // 8)
    order_tp = listed(n_tp, n_tp * TP_FIRST // 8)
    n_b = rows // LANES
    gain = norm_gain.reshape(1, chans)
    mean, scale = norm_mean.reshape(n_b, LANES), norm_scale.reshape(n_b, LANES)
    full, few = (rows, chans), (HALO, chans)

    (tail,) = call(
        tail_kernel, [(few, BF16)], [HBM, HBM],
        [pltpu.VMEM(few, BF16), pltpu.VMEM(few, BF16), pltpu.SemaphoreType.DMA((2,))],
        flops=1 << 30,
    )(glu_value, glu_gate)
    before = passed_along(tail, SP, 1)
    (taps, gated, centered, scaled, activated, conv0, act0, gain_sum, sums) = call(
        main_kernel,
        [((taps_n + 1, chans), F32), (full, BF16), (full, F32), (full, F32), (full, BF16),
         (few, F32), (few, F32), ((8, chans), F32), ((2 * n_b, LANES), F32)],
        [VMEM] * 8,
        [pltpu.VMEM((HALO + rows, chans), F32), pltpu.VMEM(full, F32)],
        flops=1 << 28,
    )(glu_value, glu_gate, conv_taps, gain, mean, scale, out_weight, out_grad)
    centered0, scaled0, gain_sum, sums, keep, send = call(
        functools.partial(first_weight_kernel, n_z=n_z, n_y=n_y),
        [(few, F32), (few, F32), ((8, chans), F32), ((n_tp, 2 * n_b, LANES), F32),
         ((n_y, n_z * half, chans), F32), ((n_y, n_z * half, chans), BF16)],
        [VMEM] * 11,
        [pltpu.VMEM((2 * HALO, chans), F32), pltpu.VMEM(few, BF16)],
        flops=1 << 28,
    )(before, conv0, act0, taps, gain, mean, scale, gain_sum, sums, out_grad, activated)
    sent = lax.ppermute(send, "z", [(i, i ^ 1) for i in range(n_z)])
    sums = exchange(sums, "tp", order_tp)
    packed, conv_grad, first_rows, value, gate = call(
        functools.partial(pack_kernel, channels=chans * n_tp, taps_n=taps_n, order=order_y),
        [((n_y, n_z * half + taps_n + 1, chans), BF16), (full, F32), (few, F32), (full, BF16),
         (full, BF16)],
        [VMEM] * 11 + [HBM] * 2,
        [pltpu.VMEM((HALO + rows, chans), F32), pltpu.SemaphoreType.DMA((2,))],
        flops=1 << 26,
    )(sums, centered, scaled, centered0, scaled0, gated, before, scale, keep, sent, gain_sum,
      glu_value, glu_gate)
    packed = exchange(packed, "y", order_y)
    (packed,) = call(
        functools.partial(middle_kernel, half=half, order=order_z),
        [((n_z, half + taps_n + 1, chans), BF16)], [VMEM], flops=1 << 22,
    )(packed)
    packed = exchange(packed, "z", order_z)
    after = passed_along(first_rows, SP, -1)
    value_grad, gate_grad = call(
        glu_kernel, [(full, BF16), (full, BF16)], [VMEM] * 4,
        [pltpu.VMEM(full, BF16), pltpu.VMEM(full, BF16), pltpu.SemaphoreType.DMA((2,))],
        flops=1 << 28, final=True, out_spec=HBM,
    )(value, gate, conv_grad, taps)
    value_grad, gate_grad = call(
        glu_end_kernel, [(full, BF16), (full, BF16)], [VMEM] * 5 + [HBM] * 2,
        [pltpu.VMEM((2 * HALO, chans), F32), pltpu.VMEM(few, BF16), pltpu.VMEM(few, BF16),
         pltpu.SemaphoreType.DMA((2,))],
        flops=1 << 24, final=True, out_spec=HBM, aliases={5: 0, 6: 1},
    )(value, gate, conv_grad, after, taps, value_grad, gate_grad)
    weight_grad, taps_grad, gain_grad = call(
        functools.partial(last_kernel, order=order_z),
        [((own, chans), F32), ((taps_n, chans), F32), ((1, chans), F32)], [VMEM], flops=1 << 22,
        final=True,
    )(packed)
    return (value_grad, gate_grad, taps_grad, gain_grad.reshape(chans), weight_grad)


def solution(mesh):
    shape = (16, 8) if mesh.shape["sp"] == 128 else (mesh.shape["sp"] // 2, 2)
    torus = Mesh(mesh.devices.reshape(*shape, mesh.shape["tp"]), ("z", "y", "tp"))
    placed = (
        P(SP, "tp"),
        P(SP, "tp"),
        P(None, "tp"),
        P("tp"),
        P(None, "tp"),
        P(SP),
        P(SP),
        P(SP, None),
    )

    return jax.shard_map(
        per_device,
        mesh=torus,
        in_specs=placed,
        out_specs=(P(SP, "tp"), P(SP, "tp"), P(None, "tp"), P("tp"), P(SP, "tp")),
        check_vma=False,
    )
```
